32 devices in a mesh: sp: 16 (over z, y, x), tp: 2 (over core).
Axes of the slice: x: 2, y: 2, z: 4, core: 2. Of those that a mesh axis runs over, the one named last changes fastest.
Arguments:
- tokens: bfloat16 [6144, 2048], P('sp', 'tp'), may hold values from -40 to 40
- mix_gain: float32 [2048], replicated, may hold values from 0.1 to 1.9
- w_pool_in: bfloat16 [2048, 1024], P(None, 'tp'), may hold values from -0.125 to 0.125
- w_qlat: bfloat16 [2048, 512], P(None, 'tp'), may hold values from -0.125 to 0.125
- w_kvlat: bfloat16 [2048, 512], P(None, 'tp'), may hold values from -0.125 to 0.125
- w_krope: bfloat16 [2048, 64], replicated, may hold values from -0.125 to 0.125
- q_gain: float32 [512], replicated, may hold values from 1 to 60
- kv_gain: float32 [512], replicated, may hold values from 0.1 to 1.9
- w_q_content: bfloat16 [512, 2048], P(None, 'tp'), may hold values from -0.25 to 0.25
- w_q_rotary: bfloat16 [512, 1024], P(None, 'tp'), may hold values from -0.25 to 0.25
- w_key: bfloat16 [512, 2048], P(None, 'tp'), may hold values from -0.25 to 0.25
- w_value: bfloat16 [512, 2048], P(None, 'tp'), may hold values from -0.25 to 0.25
- pool_mix: bfloat16 [8, 128, 128], replicated, may hold values from -0.5 to 0.5
- pool_scale: float32 [1024], replicated, may hold values from 0.1 to 1.9
- w_out_pool: bfloat16 [1024, 2048], P('tp'), may hold values from -0.109375 to 0.109375
- w_out_attn: bfloat16 [2048, 2048], P('tp'), may hold values from -0.25 to 0.25
Outputs:
- layer_out: bfloat16 [6144, 2048], P(('sp', 'tp'))
- log_total: float32 [6144, 16], P('sp', 'tp')
The draws below stay inside these ranges and needn't reach their ends.
All inputs are finite; a program needn't handle non-finite values.
Results may differ from the reference program's by a relative error of at most 0.015.
The reference program's roundings to bfloat16 on the way (of `scaled`, `weights`, `attended`, `pooled` and `pool_out`) count: a program that leaves them out, or rounds other values in their place, can miss the bound.
Values may be sent and summed in bfloat16 or wider, within the bound.
A program may use at most 64 MiB of HBM per device.

```python
import jax
import jax.numpy as jnp
from jax import lax

D = 2048
HEADS = 16
NOPE = 128
ROPE = 64
VDIM = 128
QLAT = 512
KVLAT = 512
GROUPS = 8
GROUP_DIM = 128
WIDEST = 16
SPAN = 16
TOK_DEV = 384
POOL = 1024
MIX = 3072
SEQ_LEN = 6144
SEQS = 1
TOKENS = 6144


def draw_tokens(key, part):
    base_key, column_key = jax.random.split(jax.random.fold_in(key, 11), 2)
    base = jnp.clip(jax.random.normal(base_key, (TOKENS, D), jnp.float32), -6.0, 6.0)
    ramp = jnp.arange(D, dtype=jnp.float32) / D
    column_scale = jnp.exp(jnp.log(4.0) * ramp + jax.random.uniform(column_key, (D,), jnp.float32, -0.5, 0.5))
    return jnp.clip(base * column_scale[None, :], -40.0, 40.0).astype(jnp.bfloat16)


def draw_q_gain(key, part):
    gain_key = jax.random.fold_in(key, 23)
    logs = jax.random.uniform(gain_key, (QLAT,), jnp.float32, 0.0, jnp.log(4.0))
    return jnp.exp(logs)


def steps_of(own_key, shape, cuts, least, high):
    gain, own = 1.0, jax.random.fold_in(own_key, 6)
    for axis_at, parts in cuts:
        heights = jnp.exp(jax.random.uniform(jax.random.fold_in(own, axis_at), (parts,), jnp.float32, least / len(cuts), high / len(cuts)))
        gain = gain * jnp.repeat(heights, shape[axis_at] // parts).reshape([-1 if axis == axis_at else 1 for axis in range(len(shape))])
    return gain


def normal_values(key, extent, spread, most, shards=(), kind=jnp.bfloat16):
    drawn = jax.random.normal(key, extent, jnp.float32) * spread
    if len(shards) > 0:
        drawn = steps_of(key, extent, shards, -0.22, 0.18) * drawn
    return jnp.clip(drawn, min=-most, max=most).astype(kind)


def setup_inputs(seed: int = 0) -> dict:
    keys = jax.random.split(jax.random.key(seed), 17)
    tokens = draw_tokens(jax.random.fold_in(keys[16], 71), 0)
    mix_gain = jnp.clip(1.0 + 0.18 * jax.random.normal(keys[1], (D,), jnp.float32), 0.1, 1.9)
    w_pool_in = normal_values(keys[2], (D, POOL), D ** -0.5, 0.125, ((1, 2),))
    w_qlat = normal_values(keys[3], (D, QLAT), D ** -0.5, 0.125, ((1, 2),))
    w_kvlat = normal_values(keys[4], (D, KVLAT), D ** -0.5, 0.125, ((1, 2),))
    w_krope = normal_values(keys[5], (D, ROPE), D ** -0.5, 0.125)
    q_gain = draw_q_gain(jax.random.fold_in(keys[16], 71), 0)
    kv_gain = jnp.clip(1.0 + 0.18 * jax.random.normal(keys[7], (KVLAT,), jnp.float32), 0.1, 1.9)
    w_q_content = normal_values(keys[8], (QLAT, HEADS * NOPE), QLAT ** -0.5, 0.25, ((1, 2),))
    w_q_rotary = normal_values(keys[9], (QLAT, HEADS * ROPE), QLAT ** -0.5, 0.25, ((1, 2),))
    w_key = normal_values(keys[10], (KVLAT, HEADS * NOPE), KVLAT ** -0.5, 0.25, ((1, 2),))
    w_value = normal_values(keys[11], (KVLAT, HEADS * VDIM), KVLAT ** -0.5, 0.25, ((1, 2),))
    pool_mix = normal_values(keys[12], (GROUPS, GROUP_DIM, GROUP_DIM), GROUP_DIM ** -0.5, 0.5)
    pool_scale = jnp.clip(1.0 + 0.18 * jax.random.normal(keys[13], (POOL,), jnp.float32), 0.1, 1.9)
    w_out_pool = normal_values(keys[14], (POOL, D), MIX ** -0.5, 0.109375, ((0, 2),))
    w_out_attn = normal_values(keys[15], (HEADS * VDIM, D), (HEADS * VDIM // 4) ** -0.5, 0.25, ((0, 2),))
    return {"tokens": tokens, "mix_gain": mix_gain, "w_pool_in": w_pool_in, "w_qlat": w_qlat, "w_kvlat": w_kvlat, "w_krope": w_krope, "q_gain": q_gain, "kv_gain": kv_gain, "w_q_content": w_q_content, "w_q_rotary": w_q_rotary, "w_key": w_key, "w_value": w_value, "pool_mix": pool_mix, "pool_scale": pool_scale, "w_out_pool": w_out_pool, "w_out_attn": w_out_attn}


eps_norm = 1e-06
rope_base = 10000.0
masked_score = -1e+30

def tables(positions, rotary_width):
    half_width = rotary_width // 2
    frequency = rope_base ** (-jnp.arange(half_width, dtype=jnp.float32) * 2.0 / rotary_width)
    angles = positions.astype(jnp.float32)[:, None] * frequency[None, :]
    return (jnp.cos(angles), jnp.sin(angles))

def rotate(vectors, cosine, sine_table):
    half_width = vectors.shape[-1] // 2
    first_half = vectors[..., :half_width]
    second_half = vectors[..., half_width:]
    return jnp.concatenate([first_half * cosine - second_half * sine_table, second_half * cosine + first_half * sine_table], axis=-1)

def latent_norm(latent, gain_vector):
    latent_values = latent.astype(jnp.float32)
    inverse = lax.rsqrt(lax.optimization_barrier(jnp.mean(latent_values * latent_values, axis=-1, keepdims=True)) + eps_norm)
    return (latent_values * inverse * gain_vector).astype(jnp.bfloat16)

def one_sequence(seq_tokens, mix_gain, w_pool_in, w_qlat, w_kvlat, w_krope, q_gain, kv_gain, w_q_content, w_q_rotary, w_key, w_value, pool_mix, pool_scale, w_out_pool, w_out_attn):
    length = seq_tokens.shape[0]
    positions = jnp.arange(length, dtype=jnp.int32)
    raw_values = seq_tokens.astype(jnp.float32)
    inverse_rms = lax.rsqrt(lax.optimization_barrier(jnp.mean(raw_values * raw_values, axis=1, keepdims=True)) + eps_norm)
    scaled = (raw_values * mix_gain).astype(jnp.bfloat16)

    def project(weight):
        return (jnp.dot(scaled, weight, preferred_element_type=jnp.float32) * inverse_rms).astype(jnp.bfloat16)
    pool_pre = project(w_pool_in)
    query_latent = project(w_qlat)
    kv_latent = project(w_kvlat)
    rotary_raw = project(w_krope)
    query_normed = latent_norm(query_latent, q_gain)
    key_normed = latent_norm(kv_latent, kv_gain)
    cosine, sine_table = tables(positions, ROPE)
    query_content = jnp.dot(query_normed, w_q_content, preferred_element_type=jnp.float32).astype(jnp.bfloat16).reshape(length, HEADS, NOPE)
    key_content = jnp.dot(key_normed, w_key, preferred_element_type=jnp.float32).astype(jnp.bfloat16).reshape(length, HEADS, NOPE)
    values = jnp.dot(key_normed, w_value, preferred_element_type=jnp.float32).astype(jnp.bfloat16).reshape(length, HEADS, VDIM)
    query_rotary = rotate(jnp.dot(query_normed, w_q_rotary, preferred_element_type=jnp.float32).reshape(length, HEADS, ROPE), cosine[:, None, :], sine_table[:, None, :]).astype(jnp.bfloat16)
    key_rotary = rotate(rotary_raw.astype(jnp.float32), cosine, sine_table).astype(jnp.bfloat16)
    score_scale = (NOPE + ROPE) ** (-0.5)
    key_content_wide = key_content.astype(jnp.float32)
    key_rotary_wide = key_rotary.astype(jnp.float32)
    values_wide = values.astype(jnp.float32)

    def query_block(block_index):
        row_start = block_index * TOK_DEV
        block_content = lax.dynamic_slice_in_dim(query_content, row_start, TOK_DEV, 0).astype(jnp.float32)
        block_rotary = lax.dynamic_slice_in_dim(query_rotary, row_start, TOK_DEV, 0).astype(jnp.float32)
        scores = jnp.einsum('qhd,khd->qhk', block_content, key_content_wide, precision=lax.Precision.HIGHEST)
        scores = scores + jnp.einsum('qhr,kr->qhk', block_rotary, key_rotary_wide, precision=lax.Precision.HIGHEST)
        query_positions = row_start + jnp.arange(TOK_DEV, dtype=jnp.int32)
        allowed = positions[None, None, :] <= query_positions[:, None, None]
        scores = jnp.where(allowed, scores * score_scale, masked_score)
        row_max = lax.optimization_barrier(jnp.max(scores, axis=-1))
        expo = jnp.exp(scores - row_max[..., None])
        row_total = lax.optimization_barrier(jnp.sum(expo, axis=-1))
        weights = lax.optimization_barrier(expo.astype(jnp.bfloat16))
        summed = jnp.einsum('qhk,khd->qhd', weights.astype(jnp.float32), values_wide, precision=lax.Precision.HIGHEST)
        attended = (summed / row_total[..., None]).astype(jnp.bfloat16).reshape(TOK_DEV, HEADS * VDIM)
        return (attended, row_max + jnp.log(row_total))
    attended, log_total = lax.map(query_block, jnp.arange(length // TOK_DEV))
    attended = attended.reshape(length, HEADS * VDIM)
    log_total = log_total.reshape(length, HEADS)
    pool_values = pool_pre.astype(jnp.float32)
    extended = jnp.concatenate([jnp.zeros((WIDEST - 1, POOL), jnp.float32), pool_values], axis=0)
    groups = jnp.arange(POOL, dtype=jnp.int32) // GROUP_DIM
    windows = jnp.left_shift(jnp.int32(2), groups % 4)
    window_sums = jnp.zeros((length, POOL), jnp.float32)
    for distance in range(WIDEST):
        window_sums = window_sums + jnp.where(distance < windows[None, :], extended[WIDEST - 1 - distance:WIDEST - 1 - distance + length], 0.0)
    counts = jnp.minimum(positions[:, None] + 1, windows[None, :]).astype(jnp.float32)
    pooled = lax.optimization_barrier((window_sums / counts - pool_values).astype(jnp.bfloat16))
    mixed_pool = jnp.einsum('sgc,gcd->sgd', pooled.astype(jnp.float32).reshape(length, GROUPS, GROUP_DIM), pool_mix.astype(jnp.float32), precision=lax.Precision.HIGHEST).reshape(length, POOL)
    pool_out = (mixed_pool * pool_scale).astype(jnp.bfloat16)
    layer_out = jnp.dot(pool_out, w_out_pool, preferred_element_type=jnp.float32)
    layer_out = layer_out + jnp.dot(attended, w_out_attn, preferred_element_type=jnp.float32)
    return (layer_out.astype(jnp.bfloat16), log_total)

def reference(tokens, mix_gain, w_pool_in, w_qlat, w_kvlat, w_krope, q_gain, kv_gain, w_q_content, w_q_rotary, w_key, w_value, pool_mix, pool_scale, w_out_pool, w_out_attn):
    sequences = tokens.reshape(SPAN, SEQS, TOK_DEV, D).transpose(1, 0, 2, 3).reshape(SEQS, SEQ_LEN, D)

    def per_sequence(seq_tokens):
        return one_sequence(seq_tokens, mix_gain, w_pool_in, w_qlat, w_kvlat, w_krope, q_gain, kv_gain, w_q_content, w_q_rotary, w_key, w_value, pool_mix, pool_scale, w_out_pool, w_out_attn)
    outputs, log_sums = lax.map(per_sequence, sequences)
    outputs = outputs.reshape(SEQS, SPAN, TOK_DEV, D).transpose(1, 0, 2, 3).reshape(TOKENS, D)
    log_sums = log_sums.reshape(SEQS, SPAN, TOK_DEV, HEADS).transpose(1, 0, 2, 3).reshape(TOKENS, HEADS)
    return (outputs, log_sums)
```

```python
import functools
import math
from types import SimpleNamespace

import jax
import jax.numpy as jnp
import numpy as np
from jax import lax
from jax.experimental import pallas as pl
from jax.experimental.pallas import tpu as pltpu
from jax.sharding import PartitionSpec as P

NOPE = 128
ROPE = 64
VDIM = 128
GROUP_DIM = 128
WIDEST = 16
SPAN = 16
QUAD = 4
PAIRS = SPAN // 2
LANES = 128
UNROLL = 4
MESH = pl.DeviceIdType.MESH

eps_norm = 1e-06
rope_base = 10000.0
masked_score = -1e30
f32 = jnp.float32
bf16 = jnp.bfloat16


def matmul(left, right):
    return jnp.dot(left, right, preferred_element_type=f32)


def fused_kernel(names, seq_count, *refs):
    r = SimpleNamespace(**dict(zip(names, refs)))
    tp_size, rows, own_width = r.raw.shape
    heads = r.wkv.shape[0]
    latent_width = r.wkv.shape[1]
    query_width = r.qn.shape[1]
    pool_cols = r.w_pool_v.shape[1]
    group_count = pool_cols // GROUP_DIM
    model_width = own_width * tp_size
    layers = SPAN // QUAD
    part = rows // tp_size
    scale = (NOPE + ROPE) ** (-0.5)
    factor = scale * math.log2(math.e)
    dummy = r.acc.shape[0] - 1

    place = lax.axis_index("sp")
    core = lax.axis_index("tp")
    sequence = place % seq_count
    rank = place // seq_count
    z, y, x = rank // QUAD, (rank % QUAD) // 2, rank % 2
    own_pair = rank // 2
    near_x, near_y = 1 - core % 2, core % 2
    far_x, far_y = core % 2, 1 - core % 2

    def block_at(layer, step_x, step_y):
        return layer * QUAD + ((y + step_y) % 2) * 2 + (x + step_x) % 2

    def device(block, which_core):
        return (block * seq_count + sequence, which_core)

    near = block_at(z, near_x, near_y)
    far = block_at(z, far_x, far_y)
    after = (rank + 1) % SPAN
    before = (rank + SPAN - 1) % SPAN
    friends = [device(block_at((z + up) % layers, 0, 0), core) for up in range(1, layers)]
    friends += [device(near, core), device(far, core), device(after, core), device(before, core)]
    friends += [device(rank, (core + step) % tp_size) for step in range(1, tp_size)]

    barrier = pltpu.get_barrier_semaphore()
    for friend in friends:
        pl.semaphore_signal(barrier, inc=1, device_id=friend, device_id_type=MESH)

    def load(source, target, sem):
        return pltpu.make_async_copy(source, target, sem)

    loads = {}
    own_groups = r.pool_mix.at[pl.ds(core * group_count, group_count)]
    for index, (name, source, target) in enumerate(
        [
            ("raw", r.tokens, r.raw.at[core]),
            ("kvlat", r.w_kvlat, r.w_kvlat_v),
            ("krope", r.w_krope, r.w_krope_v),
            ("qlat", r.w_qlat, r.w_qlat_v),
            ("pool", r.w_pool, r.w_pool_v),
            ("qc", r.w_qc, r.w_qc_v),
            ("qr", r.w_qr, r.w_qr_v),
            ("mix", own_groups, r.mix_v),
            ("wop", r.w_out_pool, r.w_op_v),
        ]
    ):
        loads[name] = load(source, target, r.load_sem.at[index])
        loads[name].start()
    kv_loads = []
    for head in range(heads):
        cols = slice(head * NOPE, (head + 1) * NOPE)
        kv_loads.append(load(r.w_key.at[:, cols], r.wkv.at[head, :, :NOPE], r.kv_sem.at[head, 0]))
        kv_loads.append(load(r.w_value.at[:, cols], r.wkv.at[head, :, NOPE:], r.kv_sem.at[head, 1]))
    for copy in kv_loads:
        copy.start()
    loads["woa"] = load(r.w_out_attn, r.w_oa_v, r.load_sem.at[9])
    loads["woa"].start()

    pl.semaphore_wait(barrier, len(friends))

    def remote(source, target, send, recv, where):
        return pltpu.make_async_remote_copy(
            src_ref=source, dst_ref=target, send_sem=send, recv_sem=recv,
            device_id=where, device_id_type=MESH,
        )

    def share(source, buffer, sems, step, giver):
        return remote(
            source, buffer.at[giver], sems.at[0, step - 1], sems.at[1, step - 1],
            device(rank, (core + step) % tp_size),
        )

    def giver_at(step):
        return (core + tp_size - step) % tp_size

    for step in range(1, tp_size):
        share(r.tokens, r.raw, r.tok_sem, step, core).start()

    lane = lax.broadcasted_iota(jnp.int32, (rows, LANES), 1)
    row_at = lax.broadcasted_iota(jnp.int32, (rows, LANES), 0)
    base_cos = r.base_cos[pl.ds(rank, 1), :]
    base_sin = r.base_sin[pl.ds(rank, 1), :]
    cosine = base_cos * r.step_cos[...] - base_sin * r.step_sin[...]
    sine = base_sin * r.step_cos[...] + base_cos * r.step_sin[...]
    r.cos[...] = cosine
    r.sin[...] = jnp.where(lane % ROPE < ROPE // 2, -sine, sine)
    r.bias[0] = jnp.zeros((rows, 2 * rows), f32)
    tall = lax.broadcasted_iota(jnp.int32, (rows, 2 * rows), 0)
    wide = lax.broadcasted_iota(jnp.int32, (rows, 2 * rows), 1)
    r.bias[1] = jnp.where(wide <= tall, 0.0, masked_score)
    r.bias[2] = jnp.where(wide <= tall + rows, 0.0, masked_score)
    for slot in range(UNROLL):
        r.v_scr[slot, :, VDIM:] = jnp.ones((2 * rows, LANES), bf16)

    def clear(slot, unused):
        r.peak[slot] = jnp.full((rows, LANES), masked_score, f32)
        r.acc[slot] = jnp.zeros((rows, VDIM + LANES), f32)
        return unused

    lax.fori_loop(0, dummy + 1, clear, 0)
    r.query[dummy] = jnp.zeros((rows, 2 * NOPE), bf16)

    def rotated(value):
        swapped = jnp.where(
            lane % ROPE < ROPE // 2,
            pltpu.roll(value, LANES - ROPE // 2, 1),
            pltpu.roll(value, ROPE // 2, 1),
        )
        return value * r.cos[...] + swapped * r.sin[...]

    def take_tokens(which):
        values = r.raw[which].astype(f32)
        cols = pl.ds(pl.multiple_of(which * own_width, own_width), own_width)
        r.scaled[:, cols] = (values * r.gain[which]).astype(bf16)
        return jnp.sum(values * values, axis=1, keepdims=True)

    loads["raw"].wait()
    squares = take_tokens(core)
    for step in range(1, tp_size):
        share(r.tokens, r.raw, r.tok_sem, step, giver_at(step)).wait_recv()
        squares = squares + take_tokens(giver_at(step))
    inverse_rms = lax.rsqrt(squares / model_width + eps_norm)

    def project(weight):
        return (matmul(r.scaled[...], weight) * inverse_rms).astype(bf16)

    loads["kvlat"].wait()
    r.klat[core] = project(r.w_kvlat_v[...])
    for step in range(1, tp_size):
        share(r.klat.at[core], r.klat, r.klat_sem, step, core).start()
    loads["krope"].wait()
    rotary_raw = project(r.w_krope_v[...]).astype(f32)
    key_rotary = rotated(jnp.concatenate([rotary_raw, rotary_raw], axis=1)).astype(bf16)
    r.blocks[rank, :, latent_width:] = key_rotary
    loads["qlat"].wait()
    r.qlat[core] = project(r.w_qlat_v[...])
    for step in range(1, tp_size):
        share(r.qlat.at[core], r.qlat, r.qlat_sem, step, core).start()

    def normed(latents, gain):
        pieces = [latents[which].astype(f32) for which in range(tp_size)]
        total = sum(jnp.sum(piece * piece, axis=1, keepdims=True) for piece in pieces)
        inverse = lax.rsqrt(total / gain.shape[1] + eps_norm)
        whole = pieces[0] if tp_size == 1 else jnp.concatenate(pieces, axis=1)
        return (whole * inverse * gain[...]).astype(bf16)

    for step in range(1, tp_size):
        share(r.klat.at[core], r.klat, r.klat_sem, step, giver_at(step)).wait_recv()
    r.blocks[rank, :, :latent_width] = normed(r.klat, r.kv_gain)

    def piece(block, owner):
        return r.blocks.at[block, pl.ds(pl.multiple_of(owner * part, part), part), :]

    def ici(block, send, where):
        return remote(piece(block, core), piece(block, core), send, r.ici_recv.at[block], where)

    def across(block, step):
        return remote(
            piece(block, core), piece(block, core), r.core_send.at[block, step - 1],
            r.core_recv.at[block, step - 1], device(rank, (core + step) % tp_size),
        )

    def arrival(block, step):
        return remote(
            piece(block, giver_at(step)), piece(block, giver_at(step)),
            r.core_send.at[block, step - 1], r.core_recv.at[block, step - 1],
            device(rank, giver_at(step)),
        )

    ici(rank, r.near_send.at[z], device(near, core)).start()
    ici(rank, r.far_send.at[z], device(far, core)).start()
    for up in range(1, layers):
        ici(rank, r.z_send.at[up - 1], device(block_at((z + up) % layers, 0, 0), core)).start()

    def landed(block):
        ici(block, r.near_send.at[0], device(near, core)).wait_recv()

    def hand_over(block):
        for step in range(1, tp_size):
            across(block, step).start()

    def pair_at(turn):
        return jnp.where(turn <= own_pair, own_pair - turn, turn)

    def pump(turn):
        pair = pair_at(turn)
        layer, same = pair // 2, pair % 2 == y
        column = block_at(layer, 0, 0)
        beside = block_at(layer, 1, 0)
        facing = block_at(layer, 0, 1)
        corner = block_at(layer, 1, 1)

        @pl.when(same)
        def _():
            @pl.when(layer != z)
            def _():
                landed(column)
                ici(column, r.near_send.at[layer], device(near, core)).start()
                ici(column, r.far_send.at[layer], device(far, core)).start()
                hand_over(column)

            landed(beside)

            @pl.when(near_x == 1)
            def _():
                ici(beside, r.far_send.at[layers + layer], device(far, core)).start()

            hand_over(beside)

        @pl.when(jnp.logical_not(same))
        def _():
            landed(facing)

            @pl.when(near_y == 1)
            def _():
                ici(facing, r.far_send.at[layers + layer], device(far, core)).start()

            hand_over(facing)
            landed(corner)
            hand_over(corner)

    def arrived(turn):
        pair = pair_at(turn)
        for which in range(2):
            block = 2 * pair + which

            @pl.when(block != rank)
            def _():
                for step in range(1, tp_size):
                    arrival(block, step).wait_recv()

    for step in range(1, tp_size):
        share(r.qlat.at[core], r.qlat, r.qlat_sem, step, giver_at(step)).wait_recv()
    r.qn[...] = normed(r.qlat, r.q_gain)
    loads["qc"].wait()
    loads["qr"].wait()
    for head in range(0, heads, 2):
        content = matmul(r.qn[...], r.w_qc_v[:, head * NOPE : (head + 2) * NOPE]).astype(bf16)
        turned = rotated(matmul(r.qn[...], r.w_qr_v[:, head * ROPE : (head + 2) * ROPE]))
        for which in range(2):
            r.query[head + which, :, :NOPE] = content[:, which * NOPE : (which + 1) * NOPE]
            r.query[head + which, :, NOPE:] = jnp.where(
                lane // ROPE == which, turned, 0.0
            ).astype(bf16)

    halo = WIDEST
    loads["pool"].wait()
    width = min(pool_cols, 256)
    for start in range(0, pool_cols, width):
        cols = slice(start, start + width)
        pre = project(r.w_pool_v[:, cols])
        r.ext[halo:, cols] = pre.astype(f32)
        r.rim_send[:, cols] = pre[rows - halo :]

    def rim(where):
        return remote(r.rim_send, r.rim_recv, r.rim_sem.at[0], r.rim_sem.at[1], device(where, core))

    @pl.when(rank < SPAN - 1)
    def _():
        rim(after).start()

    pump(0)

    @pl.when(rank > 0)
    def _():
        rim(before).wait_recv()
        r.ext[:halo, :] = r.rim_recv[...].astype(f32)

    @pl.when(rank == 0)
    def _():
        r.ext[:halo, :] = jnp.zeros((halo, pool_cols), f32)

    loads["mix"].wait()
    for index in range(group_count):
        cols = slice(index * GROUP_DIM, (index + 1) * GROUP_DIM)
        own = r.ext[halo:, cols]
        window = 2 ** (1 + index % 4)
        if group_count % 4:
            code = (core * group_count + index) % 4
            window = jnp.where(code == 0, 2, jnp.where(code == 1, 4, jnp.where(code == 2, 8, 16)))
        total = own
        for distance in range(1, WIDEST):
            moved = r.ext[halo - distance : halo - distance + rows, cols]
            if group_count % 4:
                total = total + moved * jnp.where(distance < window, 1.0, 0.0)
            elif distance < window:
                total = total + moved
        counts = jnp.minimum(rank * rows + row_at + 1, window).astype(f32)
        pooled = (total / counts - own).astype(bf16)
        gains = r.pool_scale[pl.ds(core * group_count + index, 1), :]
        r.pool_out[:, cols] = (matmul(pooled, r.mix_v[index]) * gains).astype(bf16)

    loads["wop"].wait()
    wide_cols = 256
    for start in range(0, model_width, wide_cols):
        cols = slice(start, start + wide_cols)
        r.y[:, cols] = matmul(r.pool_out[...], r.w_op_v[:, cols])

    pump(1)
    arrived(0)
    for copy in kv_loads:
        copy.wait()

    turns = own_pair + 1
    units = turns * heads

    def unit_of(index):
        index = jnp.minimum(index, units - 1)
        turn, head = index // heads, index % heads
        return pair_at(turn), head, head, jnp.where(turn == 0, 1 + x, 0)

    def stage_keys(index, slot):
        pair, head, query, bias = unit_of(index)
        latents = r.blocks[pl.ds(2 * pair, 2)].reshape(2 * rows, latent_width + LANES)
        both = matmul(latents[:, :latent_width], r.wkv[head]).astype(bf16)
        r.k_scr[slot, :, :NOPE] = both[:, :NOPE]
        r.k_scr[slot, :, NOPE:] = latents[:, latent_width:]
        r.v_scr[slot, :, :VDIM] = both[:, NOPE:]

    def stage_scores(index, slot, held):
        pair, head, query, bias = unit_of(index)
        scores = lax.dot_general(
            r.query[query], r.k_scr[slot], (((1,), (1,)), ((), ())), preferred_element_type=f32
        )
        r.s_scr[held] = scores + r.bias[bias]

    def stage_sums(index, slot, held):
        pair, head, query, bias = unit_of(index)
        query = jnp.where(index < units, query, dummy)
        scores = r.s_scr[held]
        old = r.peak[query]
        peak = jnp.maximum(old, jnp.max(scores, axis=1, keepdims=True))
        peaks = jnp.concatenate([peak] * (2 * rows // LANES), axis=1)
        expo = jnp.exp2((scores - peaks) * factor)
        shrink = jnp.exp2((old - peak) * factor)
        summed = matmul(expo.astype(bf16), r.v_scr[slot])
        r.acc[query] = r.acc[query] * jnp.concatenate([shrink, shrink], axis=1) + summed
        r.peak[query] = peak

    stage_keys(0, 0)
    stage_keys(1, 1)
    stage_scores(0, 0, 0)

    def needed(index):
        return jnp.minimum(index, units - 1) // heads

    def step_body(step, unused):
        first = step * UNROLL

        def bring(turn, ignored):
            @pl.when(turn < PAIRS - 1)
            def _():
                pump(turn + 1)

            arrived(turn)
            return ignored

        have = jnp.where(step == 0, 0, needed(first + 1))
        lax.fori_loop(have + 1, needed(first + UNROLL + 1) + 1, bring, 0)
        for lead in range(UNROLL):
            index = first + lead
            stage_keys(index + 2, (lead + 2) % UNROLL)
            stage_scores(index + 1, (lead + 1) % UNROLL, (lead + 1) % 2)
            stage_sums(index, lead, lead % 2)
        return unused

    lax.fori_loop(0, (units + UNROLL - 1) // UNROLL, step_body, 0)

    def relay(turn, unused):
        @pl.when(turn < PAIRS - 1)
        def _():
            pump(turn + 1)

        arrived(turn)
        return unused

    lax.fori_loop(turns, PAIRS, relay, 0)

    logs = jnp.zeros((rows, LANES), f32)
    for head in range(heads):
        total = r.acc[head, :, VDIM:]
        cols = slice(head * VDIM, (head + 1) * VDIM)
        r.attended[:, cols] = (r.acc[head, :, :VDIM] / total).astype(bf16)
        logs = jnp.where(lane == head, r.peak[head] * scale + jnp.log(total), logs)
    r.log_out[...] = logs[:, :heads]

    loads["woa"].wait()
    halves = r.give.shape[1]
    half_width = model_width // halves

    def output(which, cols):
        held = pl.ds(pl.multiple_of(which * part, part), part)
        return r.y[held, cols] + matmul(r.attended[held, :], r.w_oa_v[:, cols])

    def give(step, half):
        return remote(
            r.give.at[step - 1, half], r.take.at[step - 1, half],
            r.y_sem.at[0, step - 1, half], r.y_sem.at[1, step - 1, half],
            device(rank, (core + step) % tp_size),
        )

    for half in range(halves):
        for step in range(1, tp_size):
            for start in range(0, half_width, wide_cols):
                cols = slice(half * half_width + start, half * half_width + start + wide_cols)
                value = output((core + step) % tp_size, cols).astype(bf16)
                r.give[step - 1, half, :, start : start + wide_cols] = value
            give(step, half).start()
    own_rows = pl.ds(pl.multiple_of(core * part, part), part)
    for start in range(0, model_width, wide_cols):
        cols = slice(start, start + wide_cols)
        r.y[own_rows, cols] = output(core, cols)
    for half in range(halves):
        cols = slice(half * half_width, (half + 1) * half_width)
        value = r.y[own_rows, cols]
        for step in range(1, tp_size):
            give(step, half).wait_recv()
            value = value + r.take[step - 1, half].astype(f32)
        r.out[:, cols] = value.astype(bf16)

    for step in range(1, tp_size):
        share(r.tokens, r.raw, r.tok_sem, step, core).wait_send()
        share(r.klat.at[core], r.klat, r.klat_sem, step, core).wait_send()
        share(r.qlat.at[core], r.qlat, r.qlat_sem, step, core).wait_send()
        for half in range(halves):
            give(step, half).wait_send()

    @pl.when(rank < SPAN - 1)
    def _():
        rim(after).wait_send()

    for up in range(1, layers):
        ici(rank, r.z_send.at[up - 1], device(near, core)).wait_send()
    for layer in range(layers):
        ici(rank, r.near_send.at[layer], device(near, core)).wait_send()
    for layer in range(2 * layers):
        ici(rank, r.far_send.at[layer], device(far, core)).wait_send()

    def drain(block, unused):
        @pl.when(block != rank)
        def _():
            for step in range(1, tp_size):
                across(block, step).wait_send()

        return unused

    lax.fori_loop(0, SPAN, drain, 0)


def rotary_tables(rows):
    half_width = ROPE // 2
    frequency = rope_base ** (-np.arange(half_width, dtype=np.float64) * 2.0 / ROPE)
    frequency = np.tile(frequency, LANES // half_width)
    base = (np.arange(SPAN, dtype=np.float64) * rows)[:, None] * frequency[None, :]
    step = np.arange(rows, dtype=np.float64)[:, None] * frequency[None, :]
    return [np.asarray(t, np.float32) for t in (np.cos(base), np.sin(base), np.cos(step), np.sin(step))]


def per_device(
    tokens, mix_gain, w_pool_in, w_qlat, w_kvlat, w_krope, q_gain, kv_gain, w_q_content,
    w_q_rotary, w_key, w_value, pool_mix, pool_scale, w_out_pool, w_out_attn,
):
    tp_size = lax.axis_size("tp")
    seq_count = lax.axis_size("sp") // SPAN
    rows, own_width = tokens.shape
    model_width = own_width * tp_size
    pool_cols = w_pool_in.shape[1]
    query_width = w_q_content.shape[0]
    latent_width = w_key.shape[0]
    heads = w_key.shape[1] // NOPE
    group_count = pool_cols // GROUP_DIM
    part = rows // tp_size
    slots = heads + 1
    others = max(tp_size - 1, 1)
    layers = SPAN // QUAD
    halves = 2
    base_cos, base_sin, step_cos, step_sin = rotary_tables(rows)

    hbm = pl.BlockSpec(memory_space=pltpu.HBM)
    vmem = pl.BlockSpec(memory_space=pltpu.VMEM)
    dma = pltpu.SemaphoreType.DMA
    inputs = [
        ("tokens", tokens, hbm),
        ("w_pool", w_pool_in, hbm),
        ("w_qlat", w_qlat, hbm),
        ("w_kvlat", w_kvlat, hbm),
        ("w_krope", w_krope, hbm),
        ("w_qc", w_q_content, hbm),
        ("w_qr", w_q_rotary, hbm),
        ("w_key", w_key, hbm),
        ("w_value", w_value, hbm),
        ("pool_mix", pool_mix, hbm),
        ("w_out_pool", w_out_pool, hbm),
        ("w_out_attn", w_out_attn, hbm),
        ("gain", mix_gain.reshape(tp_size, 1, own_width), vmem),
        ("q_gain", q_gain.reshape(1, -1), vmem),
        ("kv_gain", kv_gain.reshape(1, -1), vmem),
        ("pool_scale", pool_scale.reshape(-1, GROUP_DIM), vmem),
        ("base_cos", base_cos, vmem),
        ("base_sin", base_sin, vmem),
        ("step_cos", step_cos, vmem),
        ("step_sin", step_sin, vmem),
    ]
    outputs = [
        ("out", jax.ShapeDtypeStruct((part, model_width), bf16)),
        ("log_out", jax.ShapeDtypeStruct((rows, heads), f32)),
    ]
    v = pltpu.VMEM
    scratch = [
        ("raw", v((tp_size, rows, own_width), bf16)),
        ("scaled", v((rows, model_width), bf16)),
        ("w_pool_v", v(w_pool_in.shape, bf16)),
        ("w_qlat_v", v(w_qlat.shape, bf16)),
        ("w_kvlat_v", v(w_kvlat.shape, bf16)),
        ("w_krope_v", v(w_krope.shape, bf16)),
        ("w_qc_v", v(w_q_content.shape, bf16)),
        ("w_qr_v", v(w_q_rotary.shape, bf16)),
        ("wkv", v((heads, latent_width, 2 * NOPE), bf16)),
        ("mix_v", v((group_count, GROUP_DIM, GROUP_DIM), bf16)),
        ("w_op_v", v(w_out_pool.shape, bf16)),
        ("w_oa_v", v(w_out_attn.shape, bf16)),
        ("cos", v((rows, LANES), f32)),
        ("sin", v((rows, LANES), f32)),
        ("bias", v((3, rows, 2 * rows), f32)),
        ("klat", v((tp_size,) + (rows, w_kvlat.shape[1]), bf16)),
        ("qlat", v((tp_size,) + (rows, w_qlat.shape[1]), bf16)),
        ("qn", v((rows, query_width), bf16)),
        ("blocks", v((SPAN, rows, latent_width + LANES), bf16)),
        ("query", v((slots, rows, 2 * NOPE), bf16)),
        ("acc", v((slots, rows, VDIM + LANES), f32)),
        ("peak", v((slots, rows, LANES), f32)),
        ("s_scr", v((2, rows, 2 * rows), f32)),
        ("k_scr", v((UNROLL, 2 * rows, 2 * NOPE), bf16)),
        ("v_scr", v((UNROLL, 2 * rows, VDIM + LANES), bf16)),
        ("ext", v((rows + WIDEST, pool_cols), f32)),
        ("rim_send", v((WIDEST, pool_cols), bf16)),
        ("rim_recv", v((WIDEST, pool_cols), bf16)),
        ("pool_out", v((rows, pool_cols), bf16)),
        ("attended", v((rows, heads * VDIM), bf16)),
        ("y", v((rows, model_width), f32)),
        ("give", v((others, halves, part, model_width // halves), bf16)),
        ("take", v((others, halves, part, model_width // halves), bf16)),
        ("load_sem", dma((10,))),
        ("kv_sem", dma((heads, 2))),
        ("tok_sem", dma((2, others))),
        ("klat_sem", dma((2, others))),
        ("qlat_sem", dma((2, others))),
        ("rim_sem", dma((2,))),
        ("ici_recv", dma((SPAN,))),
        ("core_send", dma((SPAN, others))),
        ("core_recv", dma((SPAN, others))),
        ("z_send", dma((layers - 1,))),
        ("near_send", dma((layers,))),
        ("far_send", dma((2 * layers,))),
        ("y_sem", dma((2, others, halves))),
    ]
    names = [entry[0] for entry in inputs + outputs + scratch]
    return pl.pallas_call(
        functools.partial(fused_kernel, names, seq_count),
        out_shape=tuple(entry[1] for entry in outputs),
        in_specs=[entry[2] for entry in inputs],
        out_specs=(vmem, vmem),
        scratch_shapes=[entry[1] for entry in scratch],
        compiler_params=pltpu.CompilerParams(
            vmem_limit_bytes=62 * 1024 * 1024, collective_id=0, has_side_effects=True
        ),
        cost_estimate=pl.CostEstimate(
            flops=30 * 10**9, bytes_accessed=2 * 10**7, transcendentals=10**7
        ),
    )(*[entry[1] for entry in inputs])


def solution(mesh):
    in_specs = (
        P("sp", "tp"),
        P(),
        P(None, "tp"),
        P(None, "tp"),
        P(None, "tp"),
        P(),
        P(),
        P(),
        P(None, "tp"),
        P(None, "tp"),
        P(None, "tp"),
        P(None, "tp"),
        P(),
        P(),
        P("tp", None),
        P("tp", None),
    )
    out_specs = (P(("sp", "tp"), None), P("sp", "tp"))
    return jax.shard_map(
        per_device, mesh=mesh, in_specs=in_specs, out_specs=out_specs, check_vma=False
    )
```

```python
import functools
import math
from types import SimpleNamespace

import jax
import jax.numpy as jnp
import numpy as np
from jax import lax
from jax.experimental import pallas as pl
from jax.experimental.pallas import tpu as pltpu
from jax.sharding import PartitionSpec as P

NOPE = 128
ROPE = 64
VDIM = 128
GROUP_DIM = 128
WIDEST = 16
SPAN = 16
QUAD = 4
PAIRS = SPAN // 2
LANES = 128
UNROLL = 4
MESH = pl.DeviceIdType.MESH

eps_norm = 1e-06
rope_base = 10000.0
masked_score = -1e30
f32 = jnp.float32
bf16 = jnp.bfloat16


def matmul(left, right):
    return jnp.dot(left, right, preferred_element_type=f32)


def fused_kernel(names, seq_count, *refs):
    r = SimpleNamespace(**dict(zip(names, refs)))
    tp_size, rows, own_width = r.raw.shape
    heads = r.wkv.shape[0]
    latent_width = r.wkv.shape[1]
    query_width = r.qn.shape[1]
    pool_cols = r.w_pool_v.shape[1]
    group_count = pool_cols // GROUP_DIM
    model_width = own_width * tp_size
    layers = SPAN // QUAD
    part = rows // tp_size
    scale = (NOPE + ROPE) ** (-0.5)
    factor = scale * math.log2(math.e)
    dummy = r.acc.shape[0] - 1

    place = lax.axis_index("sp")
    core = lax.axis_index("tp")
    sequence = place % seq_count
    rank = place // seq_count
    z, y, x = rank // QUAD, (rank % QUAD) // 2, rank % 2
    own_pair = rank // 2
    near_x, near_y = 1 - core % 2, core % 2
    far_x, far_y = core % 2, 1 - core % 2

    def block_at(layer, step_x, step_y):
        return layer * QUAD + ((y + step_y) % 2) * 2 + (x + step_x) % 2

    def device(block, which_core):
        return (block * seq_count + sequence, which_core)

    near = block_at(z, near_x, near_y)
    far = block_at(z, far_x, far_y)
    after = (rank + 1) % SPAN
    before = (rank + SPAN - 1) % SPAN
    friends = [device(block_at((z + up) % layers, 0, 0), core) for up in range(1, layers)]
    friends += [device(near, core), device(far, core), device(after, core), device(before, core)]
    friends += [device(rank, (core + step) % tp_size) for step in range(1, tp_size)]

    barrier = pltpu.get_barrier_semaphore()
    for friend in friends:
        pl.semaphore_signal(barrier, inc=1, device_id=friend, device_id_type=MESH)

    def load(source, target, sem):
        return pltpu.make_async_copy(source, target, sem)

    merged = hasattr(r, "w_lat_v")
    if merged:
        kvlat_target = r.w_lat_v.at[:, : r.klat.shape[2]]
        qlat_target = r.w_lat_v.at[:, r.klat.shape[2] :]
    else:
        kvlat_target, qlat_target = r.w_kvlat_v, r.w_qlat_v
    loads = {}
    own_groups = r.pool_mix.at[pl.ds(core * group_count, group_count)]
    for index, (name, source, target) in enumerate(
        [
            ("raw", r.tokens, r.raw.at[core]),
            ("kvlat", r.w_kvlat, kvlat_target),
            ("krope", r.w_krope, r.w_krope_v),
            ("qlat", r.w_qlat, qlat_target),
            ("pool", r.w_pool, r.w_pool_v),
            ("qc", r.w_qc, r.w_qc_v),
            ("qr", r.w_qr, r.w_qr_v),
            ("mix", own_groups, r.mix_v),
            ("wop", r.w_out_pool, r.w_op_v),
        ]
    ):
        loads[name] = load(source, target, r.load_sem.at[index])
    loads["raw"].start()
    kv_loads = []
    for head in range(heads):
        cols = slice(head * NOPE, (head + 1) * NOPE)
        kv_loads.append(load(r.w_key.at[:, cols], r.wkv.at[head, :, :NOPE], r.kv_sem.at[head, 0]))
        kv_loads.append(load(r.w_value.at[:, cols], r.wkv.at[head, :, NOPE:], r.kv_sem.at[head, 1]))
    loads["woa"] = load(r.w_out_attn, r.w_oa_v, r.load_sem.at[9])
    for name in ("kvlat", "krope", "pool", "qlat"):
        loads[name].start()
    pl.semaphore_wait(barrier, len(friends))

    def remote(source, target, send, recv, where):
        return pltpu.make_async_remote_copy(
            src_ref=source, dst_ref=target, send_sem=send, recv_sem=recv,
            device_id=where, device_id_type=MESH,
        )

    def share(source, buffer, sems, step, giver):
        return remote(
            source, buffer.at[giver], sems.at[0, step - 1], sems.at[1, step - 1],
            device(rank, (core + step) % tp_size),
        )

    def giver_at(step):
        return (core + tp_size - step) % tp_size

    for step in range(1, tp_size):
        share(r.tokens, r.raw, r.tok_sem, step, core).start()

    lane = lax.broadcasted_iota(jnp.int32, (rows, LANES), 1)
    row_at = lax.broadcasted_iota(jnp.int32, (rows, LANES), 0)
    base_cos = r.base_cos[pl.ds(rank, 1), :]
    base_sin = r.base_sin[pl.ds(rank, 1), :]
    cosine = base_cos * r.step_cos[...] - base_sin * r.step_sin[...]
    sine = base_sin * r.step_cos[...] + base_cos * r.step_sin[...]
    r.cos[...] = cosine
    r.sin[...] = jnp.where(lane % ROPE < ROPE // 2, -sine, sine)
    r.bias[0] = jnp.zeros((rows, 2 * rows), f32)
    tall = lax.broadcasted_iota(jnp.int32, (rows, 2 * rows), 0)
    wide = lax.broadcasted_iota(jnp.int32, (rows, 2 * rows), 1)
    r.bias[1] = jnp.where(wide <= tall, 0.0, masked_score)
    r.bias[2] = jnp.where(wide <= tall + rows, 0.0, masked_score)
    for slot in range(UNROLL):
        r.v_scr[slot, :, VDIM:] = jnp.ones((2 * rows, LANES), bf16)

    def clear(slot, unused):
        r.peak[slot] = jnp.full((rows, LANES), masked_score, f32)
        r.acc[slot] = jnp.zeros((rows, VDIM + LANES), f32)
        return unused

    lax.fori_loop(0, dummy + 1, clear, 0)
    r.query[dummy] = jnp.zeros((rows, 2 * NOPE), bf16)

    def rotated(value):
        swapped = jnp.where(
            lane % ROPE < ROPE // 2,
            pltpu.roll(value, LANES - ROPE // 2, 1),
            pltpu.roll(value, ROPE // 2, 1),
        )
        return value * r.cos[...] + swapped * r.sin[...]

    def take_tokens(which):
        values = r.raw[which].astype(f32)
        cols = pl.ds(pl.multiple_of(which * own_width, own_width), own_width)
        r.scaled[:, cols] = (values * r.gain[which]).astype(bf16)
        return jnp.sum(values * values, axis=1, keepdims=True)

    loads["raw"].wait()
    squares = take_tokens(core)
    for step in range(1, tp_size):
        share(r.tokens, r.raw, r.tok_sem, step, giver_at(step)).wait_recv()
        squares = squares + take_tokens(giver_at(step))
    inverse_rms = lax.rsqrt(squares / model_width + eps_norm)
    for name in ("qc", "qr", "mix", "wop"):
        loads[name].start()
    for copy in kv_loads:
        copy.start()
    loads["woa"].start()

    def project(weight):
        return (matmul(r.scaled[...], weight) * inverse_rms).astype(bf16)

    loads["kvlat"].wait()
    latent_cols, query_cols = r.klat.shape[2], r.qlat.shape[2]
    loads["qlat"].wait()
    if merged:
        latents = project(r.w_lat_v[...])
        r.klat[core] = latents[:, :latent_cols]
        r.qlat[core] = latents[:, latent_cols:]
    else:
        r.klat[core] = project(r.w_kvlat_v[...])
        r.qlat[core] = project(r.w_qlat_v[...])
    for step in range(1, tp_size):
        share(r.klat.at[core], r.klat, r.klat_sem, step, core).start()
    loads["krope"].wait()
    rotary_raw = lax.dot_general(
        r.scaled[...], r.w_krope_v[...], (((1,), (1,)), ((), ())), preferred_element_type=f32
    )
    rotary_raw = (rotary_raw * inverse_rms).astype(bf16).astype(f32)
    key_rotary = rotated(jnp.concatenate([rotary_raw, rotary_raw], axis=1)).astype(bf16)
    r.blocks[rank, :, latent_width:] = key_rotary
    halo = WIDEST
    loads["pool"].wait()
    tail_rows = matmul(r.scaled[rows - halo :, :], r.w_pool_v[...]) * inverse_rms[rows - halo :]
    r.rim_send[...] = tail_rows.astype(bf16)

    def rim(where):
        return remote(r.rim_send, r.rim_recv, r.rim_sem.at[0], r.rim_sem.at[1], device(where, core))

    @pl.when(rank < SPAN - 1)
    def _():
        rim(after).start()

    def normed(latents, gain):
        pieces = [latents[which].astype(f32) for which in range(tp_size)]
        total = sum(jnp.sum(piece * piece, axis=1, keepdims=True) for piece in pieces)
        inverse = lax.rsqrt(total / gain.shape[1] + eps_norm)
        whole = pieces[0] if tp_size == 1 else jnp.concatenate(pieces, axis=1)
        return (whole * inverse * gain[...]).astype(bf16)

    for step in range(1, tp_size):
        share(r.klat.at[core], r.klat, r.klat_sem, step, giver_at(step)).wait_recv()
    r.blocks[rank, :, :latent_width] = normed(r.klat, r.kv_gain)

    def piece(block, owner):
        return r.blocks.at[block, pl.ds(pl.multiple_of(owner * part, part), part), :]

    def ici(block, send, where):
        return remote(piece(block, core), piece(block, core), send, r.ici_recv.at[block], where)

    def across(block, step):
        return remote(
            piece(block, core), piece(block, core), r.core_send.at[block, step - 1],
            r.core_recv.at[block, step - 1], device(rank, (core + step) % tp_size),
        )

    def arrival(block, step):
        return remote(
            piece(block, giver_at(step)), piece(block, giver_at(step)),
            r.core_send.at[block, step - 1], r.core_recv.at[block, step - 1],
            device(rank, giver_at(step)),
        )

    ici(rank, r.near_send.at[z], device(near, core)).start()
    ici(rank, r.far_send.at[z], device(far, core)).start()
    def climb(block, layer):
        @pl.when(z + 1 < layers)
        def _():
            ici(block, r.z_send.at[layer], device(block_at((z + 1) % layers, 0, 0), core)).start()

    climb(rank, z)

    def landed(block):
        ici(block, r.near_send.at[0], device(near, core)).wait_recv()

    def hand_over(block):
        for step in range(1, tp_size):
            across(block, step).start()

    def columns(stage):
        @pl.when(stage < z)
        def _():
            layer = z - stage - 1
            column = block_at(layer, 0, 0)
            landed(column)
            climb(column, layer)
            ici(column, r.near_send.at[layer], device(near, core)).start()
            ici(column, r.far_send.at[layer], device(far, core)).start()
            hand_over(column)

    def sides(stage):
        @pl.when(stage <= z)
        def _():
            layer = z - stage
            beside = block_at(layer, near_x, near_y)
            landed(beside)
            ici(beside, r.far_send.at[layers + layer], device(far, core)).start()
            hand_over(beside)
            other = block_at(layer, far_x, far_y)
            landed(other)
            hand_over(other)

        @pl.when(stage > 0)
        def _():
            corner = block_at(z - stage + 1, 1, 1)
            landed(corner)
            hand_over(corner)

    def place_of(turn):
        return turn + jnp.where(turn > 0, 1 - y, 0)

    def pair_at(turn):
        at = place_of(turn)
        return (z - at // 2) * 2 + (y + at % 2) % 2

    def arrived(pair):
        for which in range(2):
            block = 2 * pair + which

            @pl.when(block != rank)
            def _():
                for step in range(1, tp_size):
                    arrival(block, step).wait_recv()

    for step in range(1, tp_size):
        share(r.qlat.at[core], r.qlat, r.qlat_sem, step, core).start()

    width = min(pool_cols, 256)
    for start in range(0, pool_cols, width):
        cols = slice(start, start + width)
        r.ext[halo:, cols] = project(r.w_pool_v[:, cols]).astype(f32)

    for step in range(1, tp_size):
        share(r.qlat.at[core], r.qlat, r.qlat_sem, step, giver_at(step)).wait_recv()
    r.qn[...] = normed(r.qlat, r.q_gain)
    loads["qc"].wait()
    loads["qr"].wait()
    for head in range(0, heads, 2):
        content = matmul(r.qn[...], r.w_qc_v[:, head * NOPE : (head + 2) * NOPE]).astype(bf16)
        turned = rotated(matmul(r.qn[...], r.w_qr_v[:, head * ROPE : (head + 2) * ROPE]))
        for which in range(2):
            r.query[head + which, :, :NOPE] = content[:, which * NOPE : (which + 1) * NOPE]
            r.query[head + which, :, NOPE:] = jnp.where(
                lane // ROPE == which, turned, 0.0
            ).astype(bf16)


    @pl.when(rank > 0)
    def _():
        rim(before).wait_recv()
        r.ext[:halo, :] = r.rim_recv[...].astype(f32)

    @pl.when(rank == 0)
    def _():
        r.ext[:halo, :] = jnp.zeros((halo, pool_cols), f32)

    loads["mix"].wait()
    for index in range(group_count):
        cols = slice(index * GROUP_DIM, (index + 1) * GROUP_DIM)
        own = r.ext[halo:, cols]
        window = 2 ** (1 + index % 4)
        if group_count % 4:
            code = (core * group_count + index) % 4
            window = jnp.where(code == 0, 2, jnp.where(code == 1, 4, jnp.where(code == 2, 8, 16)))
        total = own
        for distance in range(1, WIDEST):
            moved = r.ext[halo - distance : halo - distance + rows, cols]
            if group_count % 4:
                total = total + moved * jnp.where(distance < window, 1.0, 0.0)
            elif distance < window:
                total = total + moved
        counts = jnp.minimum(rank * rows + row_at + 1, window).astype(f32)
        pooled = (total / counts - own).astype(bf16)
        gains = r.pool_scale[pl.ds(core * group_count + index, 1), :]
        r.pool_out[:, cols] = (matmul(pooled, r.mix_v[index]) * gains).astype(bf16)

    loads["wop"].wait()
    wide_cols = 256
    for start in range(0, model_width, wide_cols):
        cols = slice(start, start + wide_cols)
        r.y[:, cols] = matmul(r.pool_out[...], r.w_op_v[:, cols])

    columns(0)
    sides(0)
    arrived(own_pair)
    for copy in kv_loads:
        copy.wait()

    turns = own_pair + 1
    units = turns * heads

    def unit_of(index):
        index = jnp.minimum(index, units - 1)
        turn, head = index // heads, index % heads
        return pair_at(turn), head, head, jnp.where(turn == 0, 1 + x, 0)

    def stage_keys(index, slot):
        pair, head, query, bias = unit_of(index)
        latents = r.blocks[pl.ds(2 * pair, 2)].reshape(2 * rows, latent_width + LANES)
        both = matmul(latents[:, :latent_width], r.wkv[head]).astype(bf16)
        r.k_scr[slot, :, :NOPE] = both[:, :NOPE]
        r.k_scr[slot, :, NOPE:] = latents[:, latent_width:]
        r.v_scr[slot, :, :VDIM] = both[:, NOPE:]

    def stage_scores(index, slot, held):
        pair, head, query, bias = unit_of(index)
        scores = lax.dot_general(
            r.query[query], r.k_scr[slot], (((1,), (1,)), ((), ())), preferred_element_type=f32
        )
        r.s_scr[held] = scores + r.bias[bias]

    def stage_sums(index, slot, held):
        pair, head, query, bias = unit_of(index)
        query = jnp.where(index < units, query, dummy)
        scores = r.s_scr[held]
        old = r.peak[query]
        peak = jnp.maximum(old, jnp.max(scores, axis=1, keepdims=True))
        peaks = jnp.concatenate([peak] * (2 * rows // LANES), axis=1)
        expo = jnp.exp2((scores - peaks) * factor)
        shrink = jnp.exp2((old - peak) * factor)
        summed = matmul(expo.astype(bf16), r.v_scr[slot])
        r.acc[query] = r.acc[query] * jnp.concatenate([shrink, shrink], axis=1) + summed
        r.peak[query] = peak

    stage_keys(0, 0)
    stage_keys(1, 1)
    stage_scores(0, 0, 0)

    def needed(index):
        return jnp.minimum(index, units - 1) // heads

    def follow(at, unused):
        @pl.when(at == 1)
        def _():
            columns(1)

        @pl.when(at % 2 == 1)
        def _():
            sides((at + 1) // 2)

        @pl.when(at % 2 == 0)
        def _():
            columns(at // 2 + 1)

        return unused

    def step_body(step, unused):
        first = step * UNROLL

        def bring(turn, ignored):
            arrived(pair_at(turn))
            return ignored

        have = jnp.where(step == 0, 0, needed(first + 1))
        seen = jnp.where(step == 0, 0, needed(first + 1 + jnp.where(step == 1, 0, UNROLL)))
        see = needed(first + UNROLL + 1 + jnp.where(step == 0, 0, UNROLL))
        lax.fori_loop(place_of(seen) + 1, place_of(see) + 1, follow, 0)
        lax.fori_loop(have + 1, needed(first + UNROLL + 1) + 1, bring, 0)
        for lead in range(UNROLL):
            index = first + lead
            stage_keys(index + 2, (lead + 2) % UNROLL)
            stage_scores(index + 1, (lead + 1) % UNROLL, (lead + 1) % 2)
            stage_sums(index, lead, lead % 2)
        return unused

    lax.fori_loop(0, (units + UNROLL - 1) // UNROLL, step_body, 0)

    lax.fori_loop(place_of(turns - 1) + 1, 2 * z + 2, follow, 0)

    @pl.when(y == 0)
    def _():
        arrived(own_pair + 1)

    logs = jnp.zeros((rows, LANES), f32)
    for head in range(heads):
        total = r.acc[head, :, VDIM:]
        cols = slice(head * VDIM, (head + 1) * VDIM)
        r.attended[:, cols] = (r.acc[head, :, :VDIM] / total).astype(bf16)
        logs = jnp.where(lane == head, r.peak[head] * scale + jnp.log(total), logs)
    r.log_out[...] = jnp.transpose(logs)[:heads]

    loads["woa"].wait()
    halves = r.give.shape[1]
    half_width = model_width // halves

    def output(which, cols):
        held = pl.ds(pl.multiple_of(which * part, part), part)
        return r.y[held, cols] + matmul(r.attended[held, :], r.w_oa_v[:, cols])

    def give(step, half):
        return remote(
            r.give.at[step - 1, half], r.take.at[step - 1, half],
            r.y_sem.at[0, step - 1, half], r.y_sem.at[1, step - 1, half],
            device(rank, (core + step) % tp_size),
        )

    for half in range(halves):
        for step in range(1, tp_size):
            for start in range(0, half_width, wide_cols):
                cols = slice(half * half_width + start, half * half_width + start + wide_cols)
                value = output((core + step) % tp_size, cols).astype(bf16)
                r.give[step - 1, half, :, start : start + wide_cols] = value
            give(step, half).start()
    own_rows = pl.ds(pl.multiple_of(core * part, part), part)
    for start in range(0, model_width, wide_cols):
        cols = slice(start, start + wide_cols)
        r.y[own_rows, cols] = output(core, cols)
    for half in range(halves):
        cols = slice(half * half_width, (half + 1) * half_width)
        value = r.y[own_rows, cols]
        for step in range(1, tp_size):
            give(step, half).wait_recv()
            value = value + r.take[step - 1, half].astype(f32)
        r.out[:, cols] = value.astype(bf16)

    for step in range(1, tp_size):
        share(r.tokens, r.raw, r.tok_sem, step, core).wait_send()
        share(r.klat.at[core], r.klat, r.klat_sem, step, core).wait_send()
        share(r.qlat.at[core], r.qlat, r.qlat_sem, step, core).wait_send()
        for half in range(halves):
            give(step, half).wait_send()

    @pl.when(rank < SPAN - 1)
    def _():
        rim(after).wait_send()

    def drain(layer, unused):
        @pl.when(z + 1 < layers)
        def _():
            ici(rank, r.z_send.at[layer], device(near, core)).wait_send()

        ici(rank, r.near_send.at[layer], device(near, core)).wait_send()
        ici(rank, r.far_send.at[layer], device(far, core)).wait_send()
        ici(rank, r.far_send.at[layers + layer], device(far, core)).wait_send()
        return unused

    lax.fori_loop(0, z + 1, drain, 0)

    def drain_across(block, unused):
        @pl.when(block != rank)
        def _():
            for step in range(1, tp_size):
                across(block, step).wait_send()

        return unused

    lax.fori_loop(0, (z + 1) * QUAD, drain_across, 0)


def rotary_tables(rows):
    half_width = ROPE // 2
    frequency = rope_base ** (-np.arange(half_width, dtype=np.float64) * 2.0 / ROPE)
    frequency = np.tile(frequency, LANES // half_width)
    base = (np.arange(SPAN, dtype=np.float64) * rows)[:, None] * frequency[None, :]
    step = np.arange(rows, dtype=np.float64)[:, None] * frequency[None, :]
    return [np.asarray(t, np.float32) for t in (np.cos(base), np.sin(base), np.cos(step), np.sin(step))]


def per_device(
    tokens, mix_gain, w_pool_in, w_qlat, w_kvlat, w_krope, q_gain, kv_gain, w_q_content,
    w_q_rotary, w_key, w_value, pool_mix, pool_scale, w_out_pool, w_out_attn,
):
    tp_size = lax.axis_size("tp")
    seq_count = lax.axis_size("sp") // SPAN
    rows, own_width = tokens.shape
    model_width = own_width * tp_size
    pool_cols = w_pool_in.shape[1]
    query_width = w_q_content.shape[0]
    latent_width = w_key.shape[0]
    heads = w_key.shape[1] // NOPE
    group_count = pool_cols // GROUP_DIM
    part = rows // tp_size
    slots = heads + 1
    others = max(tp_size - 1, 1)
    layers = SPAN // QUAD
    halves = 2
    base_cos, base_sin, step_cos, step_sin = rotary_tables(rows)

    hbm = pl.BlockSpec(memory_space=pltpu.HBM)
    vmem = pl.BlockSpec(memory_space=pltpu.VMEM)
    dma = pltpu.SemaphoreType.DMA
    inputs = [
        ("tokens", tokens, hbm),
        ("w_pool", w_pool_in, hbm),
        ("w_qlat", w_qlat, hbm),
        ("w_kvlat", w_kvlat, hbm),
        ("w_krope", w_krope.T, hbm),
        ("w_qc", w_q_content, hbm),
        ("w_qr", w_q_rotary, hbm),
        ("w_key", w_key, hbm),
        ("w_value", w_value, hbm),
        ("pool_mix", pool_mix, hbm),
        ("w_out_pool", w_out_pool, hbm),
        ("w_out_attn", w_out_attn, hbm),
        ("gain", mix_gain.reshape(tp_size, 1, own_width), vmem),
        ("q_gain", q_gain.reshape(1, -1), vmem),
        ("kv_gain", kv_gain.reshape(1, -1), vmem),
        ("pool_scale", pool_scale.reshape(-1, GROUP_DIM), vmem),
        ("base_cos", base_cos, vmem),
        ("base_sin", base_sin, vmem),
        ("step_cos", step_cos, vmem),
        ("step_sin", step_sin, vmem),
    ]
    outputs = [
        ("out", jax.ShapeDtypeStruct((part, model_width), bf16)),
        ("log_out", jax.ShapeDtypeStruct((heads, rows), f32)),
    ]
    v = pltpu.VMEM
    scratch = [
        ("raw", v((tp_size, rows, own_width), bf16)),
        ("scaled", v((rows, model_width), bf16)),
        ("w_pool_v", v(w_pool_in.shape, bf16)),
        ("w_krope_v", v(w_krope.shape[::-1], bf16)),
        ("w_qc_v", v(w_q_content.shape, bf16)),
        ("w_qr_v", v(w_q_rotary.shape, bf16)),
        ("wkv", v((heads, latent_width, 2 * NOPE), bf16)),
        ("mix_v", v((group_count, GROUP_DIM, GROUP_DIM), bf16)),
        ("w_op_v", v(w_out_pool.shape, bf16)),
        ("w_oa_v", v(w_out_attn.shape, bf16)),
        ("cos", v((rows, LANES), f32)),
        ("sin", v((rows, LANES), f32)),
        ("bias", v((3, rows, 2 * rows), f32)),
        ("klat", v((tp_size,) + (rows, w_kvlat.shape[1]), bf16)),
        ("qlat", v((tp_size,) + (rows, w_qlat.shape[1]), bf16)),
        ("qn", v((rows, query_width), bf16)),
        ("blocks", v((SPAN, rows, latent_width + LANES), bf16)),
        ("query", v((slots, rows, 2 * NOPE), bf16)),
        ("acc", v((slots, rows, VDIM + LANES), f32)),
        ("peak", v((slots, rows, LANES), f32)),
        ("s_scr", v((2, rows, 2 * rows), f32)),
        ("k_scr", v((UNROLL, 2 * rows, 2 * NOPE), bf16)),
        ("v_scr", v((UNROLL, 2 * rows, VDIM + LANES), bf16)),
        ("ext", v((rows + WIDEST, pool_cols), f32)),
        ("rim_send", v((WIDEST, pool_cols), bf16)),
        ("rim_recv", v((WIDEST, pool_cols), bf16)),
        ("pool_out", v((rows, pool_cols), bf16)),
        ("attended", v((rows, heads * VDIM), bf16)),
        ("y", v((rows, model_width), f32)),
        ("give", v((others, halves, part, model_width // halves), bf16)),
        ("take", v((others, halves, part, model_width // halves), bf16)),
        ("load_sem", dma((10,))),
        ("kv_sem", dma((heads, 2))),
        ("tok_sem", dma((2, others))),
        ("klat_sem", dma((2, others))),
        ("qlat_sem", dma((2, others))),
        ("rim_sem", dma((2,))),
        ("ici_recv", dma((SPAN,))),
        ("core_send", dma((SPAN, others))),
        ("core_recv", dma((SPAN, others))),
        ("z_send", dma((layers,))),
        ("near_send", dma((layers,))),
        ("far_send", dma((2 * layers,))),
        ("y_sem", dma((2, others, halves))),
    ]
    if w_kvlat.shape[1] % LANES == 0 and w_qlat.shape[1] % LANES == 0:
        both_cols = w_kvlat.shape[1] + w_qlat.shape[1]
        scratch.append(("w_lat_v", v((model_width, both_cols), bf16)))
    else:
        scratch.append(("w_kvlat_v", v(w_kvlat.shape, bf16)))
        scratch.append(("w_qlat_v", v(w_qlat.shape, bf16)))
    names = [entry[0] for entry in inputs + outputs + scratch]
    layer_out, log_rows = pl.pallas_call(
        functools.partial(fused_kernel, names, seq_count),
        out_shape=tuple(entry[1] for entry in outputs),
        in_specs=[entry[2] for entry in inputs],
        out_specs=(vmem, vmem),
        scratch_shapes=[entry[1] for entry in scratch],
        compiler_params=pltpu.CompilerParams(
            vmem_limit_bytes=62 * 1024 * 1024, collective_id=0, has_side_effects=True
        ),
        cost_estimate=pl.CostEstimate(
            flops=30 * 10**9, bytes_accessed=2 * 10**7, transcendentals=10**7
        ),
    )(*[entry[1] for entry in inputs])
    return layer_out, log_rows.T


def solution(mesh):
    in_specs = (
        P("sp", "tp"),
        P(),
        P(None, "tp"),
        P(None, "tp"),
        P(None, "tp"),
        P(),
        P(),
        P(),
        P(None, "tp"),
        P(None, "tp"),
        P(None, "tp"),
        P(None, "tp"),
        P(),
        P(),
        P("tp", None),
        P("tp", None),
    )
    out_specs = (P(("sp", "tp"), None), P("sp", "tp"))
    return jax.shard_map(
        per_device, mesh=mesh, in_specs=in_specs, out_specs=out_specs, check_vma=False
    )
```

```python
import functools
import math
from types import SimpleNamespace

import jax
import jax.numpy as jnp
import numpy as np
from jax import lax
from jax.experimental import pallas as pl
from jax.experimental.pallas import tpu as pltpu
from jax.sharding import PartitionSpec as P

NOPE = 128
ROPE = 64
VDIM = 128
GROUP_DIM = 128
WIDEST = 16
SPAN = 16
QUAD = 4
PAIRS = SPAN // 2
LANES = 128
UNROLL = 4
MESH = pl.DeviceIdType.MESH

eps_norm = 1e-06
rope_base = 10000.0
masked_score = -1e30
f32 = jnp.float32
bf16 = jnp.bfloat16


def matmul(left, right):
    return jnp.dot(left, right, preferred_element_type=f32)


def fused_kernel(names, seq_count, *refs):
    r = SimpleNamespace(**dict(zip(names, refs)))
    tp_size, rows, own_width = r.raw.shape
    heads = r.wkv.shape[0]
    latent_width = r.wkv.shape[1]
    query_width = r.qn.shape[1]
    pool_cols = r.w_pool_v.shape[1]
    group_count = pool_cols // GROUP_DIM
    model_width = own_width * tp_size
    layers = SPAN // QUAD
    part = rows // tp_size
    scale = (NOPE + ROPE) ** (-0.5)
    factor = scale * math.log2(math.e)
    dummy = r.acc.shape[0] - 1

    place = lax.axis_index("sp")
    core = lax.axis_index("tp")
    sequence = place % seq_count
    rank = place // seq_count
    z, y, x = rank // QUAD, (rank % QUAD) // 2, rank % 2
    own_pair = rank // 2
    near_x, near_y = 1 - core % 2, core % 2
    far_x, far_y = core % 2, 1 - core % 2

    def block_at(layer, step_x, step_y):
        return layer * QUAD + ((y + step_y) % 2) * 2 + (x + step_x) % 2

    def device(block, which_core):
        return (block * seq_count + sequence, which_core)

    near = block_at(z, near_x, near_y)
    far = block_at(z, far_x, far_y)
    after = (rank + 1) % SPAN
    before = (rank + SPAN - 1) % SPAN
    friends = [device(block_at((z + up) % layers, 0, 0), core) for up in range(1, layers)]
    friends += [device(near, core), device(far, core), device(after, core), device(before, core)]
    friends += [device(rank, (core + step) % tp_size) for step in range(1, tp_size)]

    barrier = pltpu.get_barrier_semaphore()
    for friend in friends:
        pl.semaphore_signal(barrier, inc=1, device_id=friend, device_id_type=MESH)

    def load(source, target, sem):
        return pltpu.make_async_copy(source, target, sem)

    merged = hasattr(r, "w_lat_v")
    if merged:
        kvlat_target = r.w_lat_v.at[:, : r.klat.shape[2]]
        qlat_target = r.w_lat_v.at[:, r.klat.shape[2] :]
    else:
        kvlat_target, qlat_target = r.w_kvlat_v, r.w_qlat_v
    loads = {}
    own_groups = r.pool_mix.at[pl.ds(core * group_count, group_count)]
    for index, (name, source, target) in enumerate(
        [
            ("raw", r.tokens, r.raw.at[core]),
            ("kvlat", r.w_kvlat, kvlat_target),
            ("krope", r.w_krope, r.w_krope_v),
            ("qlat", r.w_qlat, qlat_target),
            ("pool", r.w_pool, r.w_pool_v),
            ("qc", r.w_qc, r.w_qc_v),
            ("qr", r.w_qr, r.w_qr_v),
            ("mix", own_groups, r.mix_v),
            ("wop", r.w_out_pool, r.w_op_v),
        ]
    ):
        loads[name] = load(source, target, r.load_sem.at[index])
    loads["raw"].start()
    kv_loads = []
    for head in range(heads):
        cols = slice(head * NOPE, (head + 1) * NOPE)
        kv_loads.append(load(r.w_key.at[:, cols], r.wkv.at[head, :, :NOPE], r.kv_sem.at[head, 0]))
        kv_loads.append(load(r.w_value.at[:, cols], r.wkv.at[head, :, NOPE:], r.kv_sem.at[head, 1]))
    loads["woa"] = load(r.w_out_attn, r.w_oa_v, r.load_sem.at[9])
    for name in ("kvlat", "krope", "pool", "qlat"):
        loads[name].start()
    pl.semaphore_wait(barrier, len(friends))

    def remote(source, target, send, recv, where):
        return pltpu.make_async_remote_copy(
            src_ref=source, dst_ref=target, send_sem=send, recv_sem=recv,
            device_id=where, device_id_type=MESH,
        )

    def share(source, buffer, sems, step, giver):
        return remote(
            source, buffer.at[giver], sems.at[0, step - 1], sems.at[1, step - 1],
            device(rank, (core + step) % tp_size),
        )

    def giver_at(step):
        return (core + tp_size - step) % tp_size

    for step in range(1, tp_size):
        share(r.tokens, r.raw, r.tok_sem, step, core).start()

    lane = lax.broadcasted_iota(jnp.int32, (rows, LANES), 1)
    row_at = lax.broadcasted_iota(jnp.int32, (rows, LANES), 0)
    base_cos = r.base_cos[pl.ds(rank, 1), :]
    base_sin = r.base_sin[pl.ds(rank, 1), :]
    cosine = base_cos * r.step_cos[...] - base_sin * r.step_sin[...]
    sine = base_sin * r.step_cos[...] + base_cos * r.step_sin[...]
    r.cos[...] = cosine
    r.sin[...] = jnp.where(lane % ROPE < ROPE // 2, -sine, sine)
    r.bias[0] = jnp.zeros((rows, 2 * rows), f32)
    tall = lax.broadcasted_iota(jnp.int32, (rows, 2 * rows), 0)
    wide = lax.broadcasted_iota(jnp.int32, (rows, 2 * rows), 1)
    r.bias[1] = jnp.where(wide <= tall, 0.0, masked_score)
    r.bias[2] = jnp.where(wide <= tall + rows, 0.0, masked_score)
    for slot in range(UNROLL):
        r.v_scr[slot, :, VDIM:] = jnp.ones((2 * rows, LANES), bf16)

    def clear(slot, unused):
        r.peak[slot] = jnp.full((rows, LANES), masked_score, f32)
        r.acc[slot] = jnp.zeros((rows, VDIM + LANES), f32)
        return unused

    lax.fori_loop(0, dummy + 1, clear, 0)
    r.query[dummy] = jnp.zeros((rows, 2 * NOPE), bf16)

    def rotated(value):
        swapped = jnp.where(
            lane % ROPE < ROPE // 2,
            pltpu.roll(value, LANES - ROPE // 2, 1),
            pltpu.roll(value, ROPE // 2, 1),
        )
        return value * r.cos[...] + swapped * r.sin[...]

    def take_tokens(which):
        values = r.raw[which].astype(f32)
        cols = pl.ds(pl.multiple_of(which * own_width, own_width), own_width)
        r.scaled[:, cols] = (values * r.gain[which]).astype(bf16)
        return jnp.sum(values * values, axis=1, keepdims=True)

    loads["raw"].wait()
    squares = take_tokens(core)
    for step in range(1, tp_size):
        share(r.tokens, r.raw, r.tok_sem, step, giver_at(step)).wait_recv()
        squares = squares + take_tokens(giver_at(step))
    inverse_rms = lax.rsqrt(squares / model_width + eps_norm)
    for name in ("qc", "qr", "mix", "wop"):
        loads[name].start()
    for copy in kv_loads:
        copy.start()
    loads["woa"].start()

    def project(weight):
        return (matmul(r.scaled[...], weight) * inverse_rms).astype(bf16)

    loads["kvlat"].wait()
    latent_cols, query_cols = r.klat.shape[2], r.qlat.shape[2]
    loads["qlat"].wait()
    if merged:
        latents = project(r.w_lat_v[...])
        r.klat[core] = latents[:, :latent_cols]
        r.qlat[core] = latents[:, latent_cols:]
    else:
        r.klat[core] = project(r.w_kvlat_v[...])
        r.qlat[core] = project(r.w_qlat_v[...])
    for step in range(1, tp_size):
        share(r.klat.at[core], r.klat, r.klat_sem, step, core).start()
    loads["krope"].wait()
    rotary_raw = lax.dot_general(
        r.scaled[...], r.w_krope_v[...], (((1,), (1,)), ((), ())), preferred_element_type=f32
    )
    rotary_raw = (rotary_raw * inverse_rms).astype(bf16).astype(f32)
    key_rotary = rotated(jnp.concatenate([rotary_raw, rotary_raw], axis=1)).astype(bf16)
    r.blocks[rank, :, latent_width:] = key_rotary
    halo = WIDEST
    loads["pool"].wait()
    tail_rows = matmul(r.scaled[rows - halo :, :], r.w_pool_v[...]) * inverse_rms[rows - halo :]
    r.rim_send[...] = tail_rows.astype(bf16)

    def rim(where):
        return remote(r.rim_send, r.rim_recv, r.rim_sem.at[0], r.rim_sem.at[1], device(where, core))

    @pl.when(rank < SPAN - 1)
    def _():
        rim(after).start()

    def normed(latents, gain):
        pieces = [latents[which].astype(f32) for which in range(tp_size)]
        total = sum(jnp.sum(piece * piece, axis=1, keepdims=True) for piece in pieces)
        inverse = lax.rsqrt(total / gain.shape[1] + eps_norm)
        whole = pieces[0] if tp_size == 1 else jnp.concatenate(pieces, axis=1)
        return (whole * inverse * gain[...]).astype(bf16)

    for step in range(1, tp_size):
        share(r.klat.at[core], r.klat, r.klat_sem, step, giver_at(step)).wait_recv()
    r.blocks[rank, :, :latent_width] = normed(r.klat, r.kv_gain)

    def piece(block, owner):
        return r.blocks.at[block, pl.ds(pl.multiple_of(owner * part, part), part), :]

    def ici(block, send, where):
        return remote(piece(block, core), piece(block, core), send, r.ici_recv.at[block], where)

    def across(block, step):
        return remote(
            piece(block, core), piece(block, core), r.core_send.at[block, step - 1],
            r.core_recv.at[block, step - 1], device(rank, (core + step) % tp_size),
        )

    def arrival(block, step):
        return remote(
            piece(block, giver_at(step)), piece(block, giver_at(step)),
            r.core_send.at[block, step - 1], r.core_recv.at[block, step - 1],
            device(rank, giver_at(step)),
        )

    ici(rank, r.near_send.at[z], device(near, core)).start()
    ici(rank, r.far_send.at[z], device(far, core)).start()
    def climb(block, layer):
        @pl.when(z + 1 < layers)
        def _():
            ici(block, r.z_send.at[layer], device(block_at((z + 1) % layers, 0, 0), core)).start()

    climb(rank, z)

    def landed(block):
        ici(block, r.near_send.at[0], device(near, core)).wait_recv()

    def hand_over(block):
        for step in range(1, tp_size):
            across(block, step).start()

    def columns(stage):
        @pl.when(stage < z)
        def _():
            layer = z - stage - 1
            column = block_at(layer, 0, 0)
            landed(column)
            climb(column, layer)
            ici(column, r.near_send.at[layer], device(near, core)).start()
            ici(column, r.far_send.at[layer], device(far, core)).start()
            hand_over(column)

    def sides(stage):
        @pl.when(stage <= z)
        def _():
            layer = z - stage
            beside = block_at(layer, near_x, near_y)
            landed(beside)
            ici(beside, r.far_send.at[layers + layer], device(far, core)).start()
            hand_over(beside)
            other = block_at(layer, far_x, far_y)
            landed(other)
            hand_over(other)

    def corners(stage):
        corner = block_at(z - stage, 1, 1)
        landed(corner)
        hand_over(corner)

    def place_of(turn):
        return turn + jnp.where(turn > 1, 1 - y, 0)

    def pair_of(at):
        half = lax.div(at + 1, 2)
        facing = at + 1 - 2 * half
        level = half - facing
        last = level > z
        level = jnp.where(last, z, level)
        facing = jnp.where(last, 1, facing)
        facing = jnp.where(at == 0, 0, facing)
        level = jnp.where(at == 0, 0, level)
        return (z - level) * 2 + y + facing - 2 * y * facing

    def pair_at(turn):
        return pair_of(place_of(turn))

    def arrived(pair):
        for which in range(2):
            block = 2 * pair + which

            @pl.when(block != rank)
            def _():
                for step in range(1, tp_size):
                    arrival(block, step).wait_recv()

    for step in range(1, tp_size):
        share(r.qlat.at[core], r.qlat, r.qlat_sem, step, core).start()

    width = min(pool_cols, 256)
    for start in range(0, pool_cols, width):
        cols = slice(start, start + width)
        r.ext[halo:, cols] = project(r.w_pool_v[:, cols]).astype(f32)

    for step in range(1, tp_size):
        share(r.qlat.at[core], r.qlat, r.qlat_sem, step, giver_at(step)).wait_recv()
    r.qn[...] = normed(r.qlat, r.q_gain)
    loads["qc"].wait()
    loads["qr"].wait()
    for head in range(0, heads, 2):
        content = matmul(r.qn[...], r.w_qc_v[:, head * NOPE : (head + 2) * NOPE]).astype(bf16)
        turned = rotated(matmul(r.qn[...], r.w_qr_v[:, head * ROPE : (head + 2) * ROPE]))
        for which in range(2):
            r.query[head + which, :, :NOPE] = content[:, which * NOPE : (which + 1) * NOPE]
            r.query[head + which, :, NOPE:] = jnp.where(
                lane // ROPE == which, turned, 0.0
            ).astype(bf16)


    @pl.when(rank > 0)
    def _():
        rim(before).wait_recv()
        r.ext[:halo, :] = r.rim_recv[...].astype(f32)

    @pl.when(rank == 0)
    def _():
        r.ext[:halo, :] = jnp.zeros((halo, pool_cols), f32)

    loads["mix"].wait()
    for index in range(group_count):
        cols = slice(index * GROUP_DIM, (index + 1) * GROUP_DIM)
        own = r.ext[halo:, cols]
        window = 2 ** (1 + index % 4)
        if group_count % 4:
            code = (core * group_count + index) % 4
            window = jnp.where(code == 0, 2, jnp.where(code == 1, 4, jnp.where(code == 2, 8, 16)))
        total = own
        for distance in range(1, WIDEST):
            moved = r.ext[halo - distance : halo - distance + rows, cols]
            if group_count % 4:
                total = total + moved * jnp.where(distance < window, 1.0, 0.0)
            elif distance < window:
                total = total + moved
        counts = jnp.minimum(rank * rows + row_at + 1, window).astype(f32)
        pooled = (total / counts - own).astype(bf16)
        gains = r.pool_scale[pl.ds(core * group_count + index, 1), :]
        r.pool_out[:, cols] = (matmul(pooled, r.mix_v[index]) * gains).astype(bf16)

    loads["wop"].wait()
    wide_cols = 256
    for start in range(0, model_width, wide_cols):
        cols = slice(start, start + wide_cols)
        r.y[:, cols] = matmul(r.pool_out[...], r.w_op_v[:, cols])

    columns(0)
    sides(0)
    arrived(own_pair)
    for copy in kv_loads:
        copy.wait()

    turns = own_pair + 1
    units = turns * heads

    def unit_of(index):
        real = index < units
        index = jnp.minimum(index, units - 1)
        turn = lax.div(index, heads)
        head = index - turn * heads
        diagonal = jnp.where(turn == 0, 1 + x, 0)
        return pair_at(turn), head, diagonal, jnp.where(real, head, dummy)

    def stage_keys(unit, slot):
        pair, head = unit[:2]
        latents = r.blocks[pl.ds(2 * pair, 2)].reshape(2 * rows, latent_width + LANES)
        both = matmul(latents[:, :latent_width], r.wkv[head]).astype(bf16)
        r.k_scr[slot, :, :NOPE] = both[:, :NOPE]
        r.k_scr[slot, :, NOPE:] = latents[:, latent_width:]
        r.v_scr[slot, :, :VDIM] = both[:, NOPE:]

    def stage_scores(unit, slot, held):
        query, bias = unit[1:3]
        scores = lax.dot_general(
            r.query[query], r.k_scr[slot], (((1,), (1,)), ((), ())), preferred_element_type=f32
        )
        r.s_scr[held] = scores + r.bias[bias]

    def stage_sums(unit, slot, held):
        query = unit[3]
        scores = r.s_scr[held]
        old = r.peak[query]
        peak = jnp.maximum(old, jnp.max(scores, axis=1, keepdims=True))
        peaks = jnp.concatenate([peak] * (2 * rows // LANES), axis=1)
        expo = jnp.exp2((scores - peaks) * factor)
        shrink = jnp.exp2((old - peak) * factor)
        summed = matmul(expo.astype(bf16), r.v_scr[slot])
        r.acc[query] = r.acc[query] * jnp.concatenate([shrink, shrink], axis=1) + summed
        r.peak[query] = peak

    stage_keys(unit_of(0), 0)
    stage_keys(unit_of(1), 1)
    stage_scores(unit_of(0), 0, 0)

    def needed(index):
        return jnp.minimum(index, units - 1) // heads

    def follow(at, unused):
        level = (at + 1) // 2

        @pl.when(at % 2 == 1)
        def _():
            columns(level)
            sides(level)

        @pl.when(at % 2 == 0)
        def _():
            corners(level - 1)

        @pl.when(at == 2 * z + 1)
        def _():
            corners(z)

        return unused

    def step_body(step, unused):
        first = step * UNROLL

        def bring(turn, ignored):
            arrived(pair_at(turn))
            return ignored

        have = jnp.where(step == 0, 0, needed(first + 1))
        seen = jnp.where(step == 0, 0, needed(first + 1 + jnp.where(step == 1, 0, UNROLL)))
        see = needed(first + UNROLL + 1 + jnp.where(step == 0, 0, UNROLL))
        lax.fori_loop(place_of(seen) + 1, place_of(see) + 1, follow, 0)
        lax.fori_loop(have + 1, needed(first + UNROLL + 1) + 1, bring, 0)
        ahead = [unit_of(first + lead) for lead in range(UNROLL + 2)]
        for lead in range(UNROLL):
            stage_keys(ahead[lead + 2], (lead + 2) % UNROLL)
            stage_scores(ahead[lead + 1], (lead + 1) % UNROLL, (lead + 1) % 2)
            stage_sums(ahead[lead], lead, lead % 2)
        return unused

    lax.fori_loop(0, (units + UNROLL - 1) // UNROLL, step_body, 0)

    lax.fori_loop(place_of(turns - 1) + 1, 2 * z + 2, follow, 0)

    @pl.when(y == 0)
    def _():
        arrived(own_pair + 1)

    logs = jnp.zeros((rows, LANES), f32)
    for head in range(heads):
        total = r.acc[head, :, VDIM:]
        cols = slice(head * VDIM, (head + 1) * VDIM)
        r.attended[:, cols] = (r.acc[head, :, :VDIM] / total).astype(bf16)
        logs = jnp.where(lane == head, r.peak[head] * scale + jnp.log(total), logs)
    r.log_out[...] = jnp.transpose(logs)[:heads]

    loads["woa"].wait()
    halves = r.give.shape[1]
    half_width = model_width // halves

    def output(which, cols):
        held = pl.ds(pl.multiple_of(which * part, part), part)
        return r.y[held, cols] + matmul(r.attended[held, :], r.w_oa_v[:, cols])

    def give(step, half):
        return remote(
            r.give.at[step - 1, half], r.take.at[step - 1, half],
            r.y_sem.at[0, step - 1, half], r.y_sem.at[1, step - 1, half],
            device(rank, (core + step) % tp_size),
        )

    for half in range(halves):
        for step in range(1, tp_size):
            for start in range(0, half_width, wide_cols):
                cols = slice(half * half_width + start, half * half_width + start + wide_cols)
                value = output((core + step) % tp_size, cols).astype(bf16)
                r.give[step - 1, half, :, start : start + wide_cols] = value
            give(step, half).start()
    own_rows = pl.ds(pl.multiple_of(core * part, part), part)
    for start in range(0, model_width, wide_cols):
        cols = slice(start, start + wide_cols)
        r.y[own_rows, cols] = output(core, cols)
    for half in range(halves):
        cols = slice(half * half_width, (half + 1) * half_width)
        value = r.y[own_rows, cols]
        for step in range(1, tp_size):
            give(step, half).wait_recv()
            value = value + r.take[step - 1, half].astype(f32)
        r.out[:, cols] = value.astype(bf16)

    for step in range(1, tp_size):
        share(r.tokens, r.raw, r.tok_sem, step, core).wait_send()
        share(r.klat.at[core], r.klat, r.klat_sem, step, core).wait_send()
        share(r.qlat.at[core], r.qlat, r.qlat_sem, step, core).wait_send()
        for half in range(halves):
            give(step, half).wait_send()

    @pl.when(rank < SPAN - 1)
    def _():
        rim(after).wait_send()

    def drain(layer, unused):
        @pl.when(z + 1 < layers)
        def _():
            ici(rank, r.z_send.at[layer], device(near, core)).wait_send()

        ici(rank, r.near_send.at[layer], device(near, core)).wait_send()
        ici(rank, r.far_send.at[layer], device(far, core)).wait_send()
        ici(rank, r.far_send.at[layers + layer], device(far, core)).wait_send()
        return unused

    lax.fori_loop(0, z + 1, drain, 0)

    def drain_across(block, unused):
        @pl.when(block != rank)
        def _():
            for step in range(1, tp_size):
                across(block, step).wait_send()

        return unused

    lax.fori_loop(0, (z + 1) * QUAD, drain_across, 0)


def rotary_tables(rows):
    half_width = ROPE // 2
    frequency = rope_base ** (-np.arange(half_width, dtype=np.float64) * 2.0 / ROPE)
    frequency = np.tile(frequency, LANES // half_width)
    base = (np.arange(SPAN, dtype=np.float64) * rows)[:, None] * frequency[None, :]
    step = np.arange(rows, dtype=np.float64)[:, None] * frequency[None, :]
    return [np.asarray(t, np.float32) for t in (np.cos(base), np.sin(base), np.cos(step), np.sin(step))]


def per_device(
    tokens, mix_gain, w_pool_in, w_qlat, w_kvlat, w_krope, q_gain, kv_gain, w_q_content,
    w_q_rotary, w_key, w_value, pool_mix, pool_scale, w_out_pool, w_out_attn,
):
    tp_size = lax.axis_size("tp")
    seq_count = lax.axis_size("sp") // SPAN
    rows, own_width = tokens.shape
    model_width = own_width * tp_size
    pool_cols = w_pool_in.shape[1]
    query_width = w_q_content.shape[0]
    latent_width = w_key.shape[0]
    heads = w_key.shape[1] // NOPE
    group_count = pool_cols // GROUP_DIM
    part = rows // tp_size
    slots = heads + 1
    others = max(tp_size - 1, 1)
    layers = SPAN // QUAD
    halves = 2
    base_cos, base_sin, step_cos, step_sin = rotary_tables(rows)

    hbm = pl.BlockSpec(memory_space=pltpu.HBM)
    vmem = pl.BlockSpec(memory_space=pltpu.VMEM)
    dma = pltpu.SemaphoreType.DMA
    inputs = [
        ("tokens", tokens, hbm),
        ("w_pool", w_pool_in, hbm),
        ("w_qlat", w_qlat, hbm),
        ("w_kvlat", w_kvlat, hbm),
        ("w_krope", w_krope.T, hbm),
        ("w_qc", w_q_content, hbm),
        ("w_qr", w_q_rotary, hbm),
        ("w_key", w_key, hbm),
        ("w_value", w_value, hbm),
        ("pool_mix", pool_mix, hbm),
        ("w_out_pool", w_out_pool, hbm),
        ("w_out_attn", w_out_attn, hbm),
        ("gain", mix_gain.reshape(tp_size, 1, own_width), vmem),
        ("q_gain", q_gain.reshape(1, -1), vmem),
        ("kv_gain", kv_gain.reshape(1, -1), vmem),
        ("pool_scale", pool_scale.reshape(-1, GROUP_DIM), vmem),
        ("base_cos", base_cos, vmem),
        ("base_sin", base_sin, vmem),
        ("step_cos", step_cos, vmem),
        ("step_sin", step_sin, vmem),
    ]
    outputs = [
        ("out", jax.ShapeDtypeStruct((part, model_width), bf16)),
        ("log_out", jax.ShapeDtypeStruct((heads, rows), f32)),
    ]
    v = pltpu.VMEM
    scratch = [
        ("raw", v((tp_size, rows, own_width), bf16)),
        ("scaled", v((rows, model_width), bf16)),
        ("w_pool_v", v(w_pool_in.shape, bf16)),
        ("w_krope_v", v(w_krope.shape[::-1], bf16)),
        ("w_qc_v", v(w_q_content.shape, bf16)),
        ("w_qr_v", v(w_q_rotary.shape, bf16)),
        ("wkv", v((heads, latent_width, 2 * NOPE), bf16)),
        ("mix_v", v((group_count, GROUP_DIM, GROUP_DIM), bf16)),
        ("w_op_v", v(w_out_pool.shape, bf16)),
        ("w_oa_v", v(w_out_attn.shape, bf16)),
        ("cos", v((rows, LANES), f32)),
        ("sin", v((rows, LANES), f32)),
        ("bias", v((3, rows, 2 * rows), f32)),
        ("klat", v((tp_size,) + (rows, w_kvlat.shape[1]), bf16)),
        ("qlat", v((tp_size,) + (rows, w_qlat.shape[1]), bf16)),
        ("qn", v((rows, query_width), bf16)),
        ("blocks", v((SPAN, rows, latent_width + LANES), bf16)),
        ("query", v((slots, rows, 2 * NOPE), bf16)),
        ("acc", v((slots, rows, VDIM + LANES), f32)),
        ("peak", v((slots, rows, LANES), f32)),
        ("s_scr", v((2, rows, 2 * rows), f32)),
        ("k_scr", v((UNROLL, 2 * rows, 2 * NOPE), bf16)),
        ("v_scr", v((UNROLL, 2 * rows, VDIM + LANES), bf16)),
        ("ext", v((rows + WIDEST, pool_cols), f32)),
        ("rim_send", v((WIDEST, pool_cols), bf16)),
        ("rim_recv", v((WIDEST, pool_cols), bf16)),
        ("pool_out", v((rows, pool_cols), bf16)),
        ("attended", v((rows, heads * VDIM), bf16)),
        ("y", v((rows, model_width), f32)),
        ("give", v((others, halves, part, model_width // halves), bf16)),
        ("take", v((others, halves, part, model_width // halves), bf16)),
        ("load_sem", dma((10,))),
        ("kv_sem", dma((heads, 2))),
        ("tok_sem", dma((2, others))),
        ("klat_sem", dma((2, others))),
        ("qlat_sem", dma((2, others))),
        ("rim_sem", dma((2,))),
        ("ici_recv", dma((SPAN,))),
        ("core_send", dma((SPAN, others))),
        ("core_recv", dma((SPAN, others))),
        ("z_send", dma((layers,))),
        ("near_send", dma((layers,))),
        ("far_send", dma((2 * layers,))),
        ("y_sem", dma((2, others, halves))),
    ]
    if w_kvlat.shape[1] % LANES == 0 and w_qlat.shape[1] % LANES == 0:
        both_cols = w_kvlat.shape[1] + w_qlat.shape[1]
        scratch.append(("w_lat_v", v((model_width, both_cols), bf16)))
    else:
        scratch.append(("w_kvlat_v", v(w_kvlat.shape, bf16)))
        scratch.append(("w_qlat_v", v(w_qlat.shape, bf16)))
    names = [entry[0] for entry in inputs + outputs + scratch]
    layer_out, log_rows = pl.pallas_call(
        functools.partial(fused_kernel, names, seq_count),
        out_shape=tuple(entry[1] for entry in outputs),
        in_specs=[entry[2] for entry in inputs],
        out_specs=(vmem, vmem),
        scratch_shapes=[entry[1] for entry in scratch],
        compiler_params=pltpu.CompilerParams(
            vmem_limit_bytes=62 * 1024 * 1024, collective_id=0, has_side_effects=True
        ),
        cost_estimate=pl.CostEstimate(
            flops=30 * 10**9, bytes_accessed=2 * 10**7, transcendentals=10**7
        ),
    )(*[entry[1] for entry in inputs])
    return layer_out, log_rows.T


def solution(mesh):
    in_specs = (
        P("sp", "tp"),
        P(),
        P(None, "tp"),
        P(None, "tp"),
        P(None, "tp"),
        P(),
        P(),
        P(),
        P(None, "tp"),
        P(None, "tp"),
        P(None, "tp"),
        P(None, "tp"),
        P(),
        P(),
        P("tp", None),
        P("tp", None),
    )
    out_specs = (P(("sp", "tp"), None), P("sp", "tp"))
    return jax.shard_map(
        per_device, mesh=mesh, in_specs=in_specs, out_specs=out_specs, check_vma=False
    )
```

```python
import functools
import math
from types import SimpleNamespace

import jax
import jax.numpy as jnp
import numpy as np
from jax import lax
from jax.experimental import pallas as pl
from jax.experimental.pallas import tpu as pltpu
from jax.sharding import PartitionSpec as P

NOPE = 128
ROPE = 64
VDIM = 128
GROUP_DIM = 128
WIDEST = 16
SPAN = 16
QUAD = 4
PAIRS = SPAN // 2
LANES = 128
UNROLL = 4
MESH = pl.DeviceIdType.MESH

eps_norm = 1e-06
rope_base = 10000.0
masked_score = -1e30
f32 = jnp.float32
bf16 = jnp.bfloat16


def matmul(left, right):
    return jnp.dot(left, right, preferred_element_type=f32)


def fused_kernel(names, seq_count, *refs):
    r = SimpleNamespace(**dict(zip(names, refs)))
    tp_size, rows, own_width = r.raw.shape
    heads = r.wkv.shape[0]
    latent_width = r.wkv.shape[1]
    query_width = r.qn.shape[1]
    pool_cols = r.w_pool_v.shape[1]
    group_count = pool_cols // GROUP_DIM
    model_width = own_width * tp_size
    layers = SPAN // QUAD
    part = rows // tp_size
    scale = (NOPE + ROPE) ** (-0.5)
    factor = scale * math.log2(math.e)
    dummy = r.acc.shape[0] - 1

    place = lax.axis_index("sp")
    core = lax.axis_index("tp")
    sequence = place % seq_count
    rank = place // seq_count
    z, y, x = rank // QUAD, (rank % QUAD) // 2, rank % 2
    own_pair = rank // 2
    near_x, near_y = 1 - core % 2, core % 2
    far_x, far_y = core % 2, 1 - core % 2

    def block_at(layer, step_x, step_y):
        return layer * QUAD + ((y + step_y) % 2) * 2 + (x + step_x) % 2

    def device(block, which_core):
        return (block * seq_count + sequence, which_core)

    near = block_at(z, near_x, near_y)
    far = block_at(z, far_x, far_y)
    after = (rank + 1) % SPAN
    before = (rank + SPAN - 1) % SPAN
    friends = [device(block_at((z + up) % layers, 0, 0), core) for up in range(1, layers)]
    friends += [device(near, core), device(far, core), device(after, core), device(before, core)]
    friends += [device(rank, (core + step) % tp_size) for step in range(1, tp_size)]

    barrier = pltpu.get_barrier_semaphore()
    for friend in friends:
        pl.semaphore_signal(barrier, inc=1, device_id=friend, device_id_type=MESH)

    def load(source, target, sem):
        return pltpu.make_async_copy(source, target, sem)

    merged = hasattr(r, "w_lat_v")
    if merged:
        kvlat_target = r.w_lat_v.at[:, : r.klat.shape[2]]
        qlat_target = r.w_lat_v.at[:, r.klat.shape[2] :]
    else:
        kvlat_target, qlat_target = r.w_kvlat_v, r.w_qlat_v
    loads = {}
    own_groups = r.pool_mix.at[pl.ds(core * group_count, group_count)]
    for index, (name, source, target) in enumerate(
        [
            ("raw", r.tokens, r.raw.at[core]),
            ("kvlat", r.w_kvlat, kvlat_target),
            ("krope", r.w_krope, r.w_krope_v),
            ("qlat", r.w_qlat, qlat_target),
            ("pool", r.w_pool, r.w_pool_v),
            ("qc", r.w_qc, r.w_qc_v),
            ("qr", r.w_qr, r.w_qr_v),
            ("mix", own_groups, r.mix_v),
            ("wop", r.w_out_pool, r.w_op_v),
        ]
    ):
        loads[name] = load(source, target, r.load_sem.at[index])
    loads["raw"].start()
    kv_loads = []
    for head in range(heads):
        cols = slice(head * NOPE, (head + 1) * NOPE)
        kv_loads.append(load(r.w_key.at[:, cols], r.wkv.at[head, :, :NOPE], r.kv_sem.at[head, 0]))
        kv_loads.append(load(r.w_value.at[:, cols], r.wkv.at[head, :, NOPE:], r.kv_sem.at[head, 1]))
    loads["woa"] = load(r.w_out_attn, r.w_oa_v, r.load_sem.at[9])
    for name in ("kvlat", "krope", "pool", "qlat"):
        loads[name].start()
    pl.semaphore_wait(barrier, len(friends))

    def remote(source, target, send, recv, where):
        return pltpu.make_async_remote_copy(
            src_ref=source, dst_ref=target, send_sem=send, recv_sem=recv,
            device_id=where, device_id_type=MESH,
        )

    def share(source, buffer, sems, step, giver):
        return remote(
            source, buffer.at[giver], sems.at[0, step - 1], sems.at[1, step - 1],
            device(rank, (core + step) % tp_size),
        )

    def giver_at(step):
        return (core + tp_size - step) % tp_size

    for step in range(1, tp_size):
        share(r.tokens, r.raw, r.tok_sem, step, core).start()

    lane = lax.broadcasted_iota(jnp.int32, (rows, LANES), 1)
    row_at = lax.broadcasted_iota(jnp.int32, (rows, LANES), 0)
    base_cos = r.base_cos[pl.ds(rank, 1), :]
    base_sin = r.base_sin[pl.ds(rank, 1), :]
    cosine = base_cos * r.step_cos[...] - base_sin * r.step_sin[...]
    sine = base_sin * r.step_cos[...] + base_cos * r.step_sin[...]
    r.cos[...] = cosine
    r.sin[...] = jnp.where(lane % ROPE < ROPE // 2, -sine, sine)
    r.bias[0] = jnp.zeros((rows, 2 * rows), f32)
    tall = lax.broadcasted_iota(jnp.int32, (rows, 2 * rows), 0)
    wide = lax.broadcasted_iota(jnp.int32, (rows, 2 * rows), 1)
    r.bias[1] = jnp.where(wide <= tall, 0.0, masked_score)
    r.bias[2] = jnp.where(wide <= tall + rows, 0.0, masked_score)
    for slot in range(UNROLL):
        r.v_scr[slot, :, VDIM:] = jnp.ones((2 * rows, LANES), bf16)

    def clear(slot, unused):
        r.peak[slot] = jnp.full((rows, LANES), masked_score, f32)
        r.acc[slot] = jnp.zeros((rows, VDIM + LANES), f32)
        return unused

    lax.fori_loop(0, dummy + 1, clear, 0)
    r.query[dummy] = jnp.zeros((rows, 2 * NOPE), bf16)

    def rotated(value):
        swapped = jnp.where(
            lane % ROPE < ROPE // 2,
            pltpu.roll(value, LANES - ROPE // 2, 1),
            pltpu.roll(value, ROPE // 2, 1),
        )
        return value * r.cos[...] + swapped * r.sin[...]

    def take_tokens(which):
        values = r.raw[which].astype(f32)
        cols = pl.ds(pl.multiple_of(which * own_width, own_width), own_width)
        r.scaled[:, cols] = (values * r.gain[which]).astype(bf16)
        return jnp.sum(values * values, axis=1, keepdims=True)

    loads["raw"].wait()
    squares = take_tokens(core)
    for step in range(1, tp_size):
        share(r.tokens, r.raw, r.tok_sem, step, giver_at(step)).wait_recv()
        squares = squares + take_tokens(giver_at(step))
    inverse_rms = lax.rsqrt(squares / model_width + eps_norm)
    for name in ("qc", "qr", "mix", "wop"):
        loads[name].start()
    for copy in kv_loads:
        copy.start()
    loads["woa"].start()

    def project(weight):
        return (matmul(r.scaled[...], weight) * inverse_rms).astype(bf16)

    loads["kvlat"].wait()
    latent_cols, query_cols = r.klat.shape[2], r.qlat.shape[2]
    loads["qlat"].wait()
    if merged:
        latents = project(r.w_lat_v[...])
        r.klat[core] = latents[:, :latent_cols]
        r.qlat[core] = latents[:, latent_cols:]
    else:
        r.klat[core] = project(r.w_kvlat_v[...])
        r.qlat[core] = project(r.w_qlat_v[...])
    for step in range(1, tp_size):
        share(r.klat.at[core], r.klat, r.klat_sem, step, core).start()
    loads["krope"].wait()
    rotary_raw = lax.dot_general(
        r.scaled[...], r.w_krope_v[...], (((1,), (1,)), ((), ())), preferred_element_type=f32
    )
    rotary_raw = (rotary_raw * inverse_rms).astype(bf16).astype(f32)
    key_rotary = rotated(jnp.concatenate([rotary_raw, rotary_raw], axis=1)).astype(bf16)
    r.blocks[rank, :, latent_width:] = key_rotary
    halo = WIDEST
    loads["pool"].wait()
    tail_rows = matmul(r.scaled[rows - halo :, :], r.w_pool_v[...]) * inverse_rms[rows - halo :]
    r.rim_send[...] = tail_rows.astype(bf16)

    def rim(where):
        return remote(r.rim_send, r.rim_recv, r.rim_sem.at[0], r.rim_sem.at[1], device(where, core))

    @pl.when(rank < SPAN - 1)
    def _():
        rim(after).start()

    def normed(latents, gain):
        pieces = [latents[which].astype(f32) for which in range(tp_size)]
        total = sum(jnp.sum(piece * piece, axis=1, keepdims=True) for piece in pieces)
        inverse = lax.rsqrt(total / gain.shape[1] + eps_norm)
        whole = pieces[0] if tp_size == 1 else jnp.concatenate(pieces, axis=1)
        return (whole * inverse * gain[...]).astype(bf16)

    for step in range(1, tp_size):
        share(r.klat.at[core], r.klat, r.klat_sem, step, giver_at(step)).wait_recv()
    r.blocks[rank, :, :latent_width] = normed(r.klat, r.kv_gain)

    def piece(block, owner):
        return r.blocks.at[block, pl.ds(pl.multiple_of(owner * part, part), part), :]

    def ici(block, send, where):
        return remote(piece(block, core), piece(block, core), send, r.ici_recv.at[block], where)

    def across(block, step):
        return remote(
            piece(block, core), piece(block, core), r.core_send.at[block, step - 1],
            r.core_recv.at[block, step - 1], device(rank, (core + step) % tp_size),
        )

    def arrival(block, step):
        return remote(
            piece(block, giver_at(step)), piece(block, giver_at(step)),
            r.core_send.at[block, step - 1], r.core_recv.at[block, step - 1],
            device(rank, giver_at(step)),
        )

    ici(rank, r.near_send.at[z], device(near, core)).start()
    ici(rank, r.far_send.at[z], device(far, core)).start()
    def climb(block, layer):
        @pl.when(z + 1 < layers)
        def _():
            ici(block, r.z_send.at[layer], device(block_at((z + 1) % layers, 0, 0), core)).start()

    climb(rank, z)

    def landed(block):
        ici(block, r.near_send.at[0], device(near, core)).wait_recv()

    def hand_over(block):
        for step in range(1, tp_size):
            across(block, step).start()

    def columns(stage):
        @pl.when(stage < z)
        def _():
            layer = z - stage - 1
            column = block_at(layer, 0, 0)
            landed(column)
            climb(column, layer)
            ici(column, r.near_send.at[layer], device(near, core)).start()
            ici(column, r.far_send.at[layer], device(far, core)).start()
            hand_over(column)

    def sides(stage):
        @pl.when(stage <= z)
        def _():
            layer = z - stage
            beside = block_at(layer, near_x, near_y)
            landed(beside)
            ici(beside, r.far_send.at[layers + layer], device(far, core)).start()
            hand_over(beside)
            other = block_at(layer, far_x, far_y)
            landed(other)
            hand_over(other)

    def corners(stage):
        corner = block_at(z - stage, 1, 1)
        landed(corner)
        hand_over(corner)

    def place_of(turn):
        return turn + jnp.where(turn > 1, 1 - y, 0)

    def pair_of(at):
        half = lax.div(at + 1, 2)
        facing = at + 1 - 2 * half
        level = half - facing
        last = level > z
        level = jnp.where(last, z, level)
        facing = jnp.where(last, 1, facing)
        facing = jnp.where(at == 0, 0, facing)
        level = jnp.where(at == 0, 0, level)
        return (z - level) * 2 + y + facing - 2 * y * facing

    def pair_at(turn):
        return pair_of(place_of(turn))

    def arrived(pair):
        for which in range(2):
            block = 2 * pair + which

            @pl.when(block != rank)
            def _():
                for step in range(1, tp_size):
                    arrival(block, step).wait_recv()

    for step in range(1, tp_size):
        share(r.qlat.at[core], r.qlat, r.qlat_sem, step, core).start()

    width = min(pool_cols, 256)
    for start in range(0, pool_cols, width):
        cols = slice(start, start + width)
        r.ext[halo:, cols] = project(r.w_pool_v[:, cols]).astype(f32)

    for step in range(1, tp_size):
        share(r.qlat.at[core], r.qlat, r.qlat_sem, step, giver_at(step)).wait_recv()
    r.qn[...] = normed(r.qlat, r.q_gain)
    loads["qc"].wait()
    loads["qr"].wait()
    for head in range(0, heads, 2):
        content = matmul(r.qn[...], r.w_qc_v[:, head * NOPE : (head + 2) * NOPE]).astype(bf16)
        turned = rotated(matmul(r.qn[...], r.w_qr_v[:, head * ROPE : (head + 2) * ROPE]))
        for which in range(2):
            r.query[head + which, :, :NOPE] = content[:, which * NOPE : (which + 1) * NOPE]
            r.query[head + which, :, NOPE:] = jnp.where(
                lane // ROPE == which, turned, 0.0
            ).astype(bf16)


    @pl.when(rank > 0)
    def _():
        rim(before).wait_recv()
        r.ext[:halo, :] = r.rim_recv[...].astype(f32)

    @pl.when(rank == 0)
    def _():
        r.ext[:halo, :] = jnp.zeros((halo, pool_cols), f32)

    loads["mix"].wait()
    for index in range(group_count):
        cols = slice(index * GROUP_DIM, (index + 1) * GROUP_DIM)
        own = r.ext[halo:, cols]
        window = 2 ** (1 + index % 4)
        if group_count % 4:
            code = (core * group_count + index) % 4
            window = jnp.where(code == 0, 2, jnp.where(code == 1, 4, jnp.where(code == 2, 8, 16)))
        total = own
        for distance in range(1, WIDEST):
            moved = r.ext[halo - distance : halo - distance + rows, cols]
            if group_count % 4:
                total = total + moved * jnp.where(distance < window, 1.0, 0.0)
            elif distance < window:
                total = total + moved
        counts = jnp.minimum(rank * rows + row_at + 1, window).astype(f32)
        pooled = (total / counts - own).astype(bf16)
        gains = r.pool_scale[pl.ds(core * group_count + index, 1), :]
        r.pool_out[:, cols] = (matmul(pooled, r.mix_v[index]) * gains).astype(bf16)

    loads["wop"].wait()
    wide_cols = 256
    for start in range(0, model_width, wide_cols):
        cols = slice(start, start + wide_cols)
        r.y[:, cols] = matmul(r.pool_out[...], r.w_op_v[:, cols])

    columns(0)
    sides(0)
    arrived(own_pair)
    for copy in kv_loads:
        copy.wait()

    turns = own_pair + 1
    units = turns * heads

    def unit_of(index):
        real = index < units
        index = jnp.minimum(index, units - 1)
        turn = lax.div(index, heads)
        head = index - turn * heads
        diagonal = jnp.where(turn == 0, 1 + x, 0)
        return pair_at(turn), head, diagonal, jnp.where(real, head, dummy)

    def stage_keys(unit, slot):
        pair, head = unit[:2]
        latents = r.blocks[pl.ds(2 * pair, 2)].reshape(2 * rows, latent_width + LANES)
        both = matmul(latents[:, :latent_width], r.wkv[head]).astype(bf16)
        r.k_scr[slot, :, :NOPE] = both[:, :NOPE]
        r.k_scr[slot, :, NOPE:] = latents[:, latent_width:]
        r.v_scr[slot, :, :VDIM] = both[:, NOPE:]

    def stage_scores(unit, slot, held):
        query, bias = unit[1:3]
        scores = lax.dot_general(
            r.query[query], r.k_scr[slot], (((1,), (1,)), ((), ())), preferred_element_type=f32
        )
        r.s_scr[held] = scores + r.bias[bias]

    def stage_sums(unit, slot, held):
        query = unit[3]
        scores = r.s_scr[held]
        old = r.peak[query]
        peak = jnp.maximum(old, jnp.max(scores, axis=1, keepdims=True))
        peaks = jnp.concatenate([peak] * (2 * rows // LANES), axis=1)
        expo = jnp.exp2((scores - peaks) * factor)
        shrink = jnp.exp2((old - peak) * factor)
        summed = matmul(expo.astype(bf16), r.v_scr[slot])
        r.acc[query] = r.acc[query] * jnp.concatenate([shrink, shrink], axis=1) + summed
        r.peak[query] = peak

    stage_keys(unit_of(0), 0)
    stage_keys(unit_of(1), 1)
    stage_scores(unit_of(0), 0, 0)

    def needed(index):
        return jnp.minimum(index, units - 1) // heads

    def follow(at, unused):
        level = (at + 1) // 2

        @pl.when(at % 2 == 1)
        def _():
            columns(level)
            sides(level)

        @pl.when(at % 2 == 0)
        def _():
            corners(level - 1)

        @pl.when(at == 2 * z + 1)
        def _():
            corners(z)

        return unused

    def step_body(step, unused):
        first = step * UNROLL

        def bring(turn, ignored):
            arrived(pair_at(turn))
            return ignored

        have = jnp.where(step == 0, 0, needed(first + 1))
        seen = jnp.where(step == 0, 0, needed(first + 1 + jnp.where(step == 1, 0, UNROLL)))
        see = needed(first + UNROLL + 1 + jnp.where(step == 0, 0, UNROLL))
        lax.fori_loop(place_of(seen) + 1, place_of(see) + 1, follow, 0)
        lax.fori_loop(have + 1, needed(first + UNROLL + 1) + 1, bring, 0)
        ahead = [unit_of(first + lead) for lead in range(UNROLL + 2)]
        for lead in range(UNROLL):
            stage_keys(ahead[lead + 2], (lead + 2) % UNROLL)
            stage_scores(ahead[lead + 1], (lead + 1) % UNROLL, (lead + 1) % 2)
            stage_sums(ahead[lead], lead, lead % 2)
        return unused

    lax.fori_loop(0, (units + UNROLL - 1) // UNROLL, step_body, 0)

    lax.fori_loop(place_of(turns - 1) + 1, 2 * z + 2, follow, 0)

    @pl.when(y == 0)
    def _():
        arrived(own_pair + 1)

    logs = jnp.zeros((rows, LANES), f32)
    for head in range(heads):
        total = r.acc[head, :, VDIM:]
        cols = slice(head * VDIM, (head + 1) * VDIM)
        r.attended[:, cols] = (r.acc[head, :, :VDIM] / total).astype(bf16)
        logs = jnp.where(lane == head, r.peak[head] * scale + jnp.log(total), logs)
    r.log_out[...] = jnp.transpose(logs)[:heads]

    loads["woa"].wait()
    halves = r.give.shape[1]
    half_width = model_width // halves

    def output(which, cols):
        held = pl.ds(pl.multiple_of(which * part, part), part)
        return r.y[held, cols] + matmul(r.attended[held, :], r.w_oa_v[:, cols])

    def give(step, half):
        return remote(
            r.give.at[step - 1, half], r.take.at[step - 1, half],
            r.y_sem.at[0, step - 1, half], r.y_sem.at[1, step - 1, half],
            device(rank, (core + step) % tp_size),
        )

    for half in range(halves):
        for step in range(1, tp_size):
            for start in range(0, half_width, wide_cols):
                cols = slice(half * half_width + start, half * half_width + start + wide_cols)
                value = output((core + step) % tp_size, cols).astype(bf16)
                r.give[step - 1, half, :, start : start + wide_cols] = value
            give(step, half).start()
    own_rows = pl.ds(pl.multiple_of(core * part, part), part)
    for start in range(0, model_width, wide_cols):
        cols = slice(start, start + wide_cols)
        r.y[own_rows, cols] = output(core, cols)
    for half in range(halves):
        cols = slice(half * half_width, (half + 1) * half_width)
        value = r.y[own_rows, cols]
        for step in range(1, tp_size):
            give(step, half).wait_recv()
            value = value + r.take[step - 1, half].astype(f32)
        r.out[:, cols] = value

    for step in range(1, tp_size):
        share(r.tokens, r.raw, r.tok_sem, step, core).wait_send()
        share(r.klat.at[core], r.klat, r.klat_sem, step, core).wait_send()
        share(r.qlat.at[core], r.qlat, r.qlat_sem, step, core).wait_send()
        for half in range(halves):
            give(step, half).wait_send()

    @pl.when(rank < SPAN - 1)
    def _():
        rim(after).wait_send()

    def drain(layer, unused):
        @pl.when(z + 1 < layers)
        def _():
            ici(rank, r.z_send.at[layer], device(near, core)).wait_send()

        ici(rank, r.near_send.at[layer], device(near, core)).wait_send()
        ici(rank, r.far_send.at[layer], device(far, core)).wait_send()
        ici(rank, r.far_send.at[layers + layer], device(far, core)).wait_send()
        return unused

    lax.fori_loop(0, z + 1, drain, 0)

    def drain_across(block, unused):
        @pl.when(block != rank)
        def _():
            for step in range(1, tp_size):
                across(block, step).wait_send()

        return unused

    lax.fori_loop(0, (z + 1) * QUAD, drain_across, 0)


def rotary_tables(rows):
    half_width = ROPE // 2
    frequency = rope_base ** (-np.arange(half_width, dtype=np.float64) * 2.0 / ROPE)
    frequency = np.tile(frequency, LANES // half_width)
    base = (np.arange(SPAN, dtype=np.float64) * rows)[:, None] * frequency[None, :]
    step = np.arange(rows, dtype=np.float64)[:, None] * frequency[None, :]
    return [np.asarray(t, np.float32) for t in (np.cos(base), np.sin(base), np.cos(step), np.sin(step))]


def per_device(
    tokens, mix_gain, w_pool_in, w_qlat, w_kvlat, w_krope, q_gain, kv_gain, w_q_content,
    w_q_rotary, w_key, w_value, pool_mix, pool_scale, w_out_pool, w_out_attn,
):
    tp_size = lax.axis_size("tp")
    seq_count = lax.axis_size("sp") // SPAN
    rows, own_width = tokens.shape
    model_width = own_width * tp_size
    pool_cols = w_pool_in.shape[1]
    query_width = w_q_content.shape[0]
    latent_width = w_key.shape[0]
    heads = w_key.shape[1] // NOPE
    group_count = pool_cols // GROUP_DIM
    part = rows // tp_size
    slots = heads + 1
    others = max(tp_size - 1, 1)
    layers = SPAN // QUAD
    halves = 2
    base_cos, base_sin, step_cos, step_sin = rotary_tables(rows)

    hbm = pl.BlockSpec(memory_space=pltpu.HBM)
    vmem = pl.BlockSpec(memory_space=pltpu.VMEM)
    dma = pltpu.SemaphoreType.DMA
    inputs = [
        ("tokens", tokens, hbm),
        ("w_pool", w_pool_in, hbm),
        ("w_qlat", w_qlat, hbm),
        ("w_kvlat", w_kvlat, hbm),
        ("w_krope", w_krope.T, hbm),
        ("w_qc", w_q_content, hbm),
        ("w_qr", w_q_rotary, hbm),
        ("w_key", w_key, hbm),
        ("w_value", w_value, hbm),
        ("pool_mix", pool_mix, hbm),
        ("w_out_pool", w_out_pool, hbm),
        ("w_out_attn", w_out_attn, hbm),
        ("gain", mix_gain.reshape(tp_size, 1, own_width), vmem),
        ("q_gain", q_gain.reshape(1, -1), vmem),
        ("kv_gain", kv_gain.reshape(1, -1), vmem),
        ("pool_scale", pool_scale.reshape(-1, GROUP_DIM), vmem),
        ("base_cos", base_cos, vmem),
        ("base_sin", base_sin, vmem),
        ("step_cos", step_cos, vmem),
        ("step_sin", step_sin, vmem),
    ]
    outputs = [
        ("out", jax.ShapeDtypeStruct((part, model_width), f32)),
        ("log_out", jax.ShapeDtypeStruct((heads, rows), f32)),
    ]
    v = pltpu.VMEM
    scratch = [
        ("raw", v((tp_size, rows, own_width), bf16)),
        ("scaled", v((rows, model_width), bf16)),
        ("w_pool_v", v(w_pool_in.shape, bf16)),
        ("w_krope_v", v(w_krope.shape[::-1], bf16)),
        ("w_qc_v", v(w_q_content.shape, bf16)),
        ("w_qr_v", v(w_q_rotary.shape, bf16)),
        ("wkv", v((heads, latent_width, 2 * NOPE), bf16)),
        ("mix_v", v((group_count, GROUP_DIM, GROUP_DIM), bf16)),
        ("w_op_v", v(w_out_pool.shape, bf16)),
        ("w_oa_v", v(w_out_attn.shape, bf16)),
        ("cos", v((rows, LANES), f32)),
        ("sin", v((rows, LANES), f32)),
        ("bias", v((3, rows, 2 * rows), f32)),
        ("klat", v((tp_size,) + (rows, w_kvlat.shape[1]), bf16)),
        ("qlat", v((tp_size,) + (rows, w_qlat.shape[1]), bf16)),
        ("qn", v((rows, query_width), bf16)),
        ("blocks", v((SPAN, rows, latent_width + LANES), bf16)),
        ("query", v((slots, rows, 2 * NOPE), bf16)),
        ("acc", v((slots, rows, VDIM + LANES), f32)),
        ("peak", v((slots, rows, LANES), f32)),
        ("s_scr", v((2, rows, 2 * rows), f32)),
        ("k_scr", v((UNROLL, 2 * rows, 2 * NOPE), bf16)),
        ("v_scr", v((UNROLL, 2 * rows, VDIM + LANES), bf16)),
        ("ext", v((rows + WIDEST, pool_cols), f32)),
        ("rim_send", v((WIDEST, pool_cols), bf16)),
        ("rim_recv", v((WIDEST, pool_cols), bf16)),
        ("pool_out", v((rows, pool_cols), bf16)),
        ("attended", v((rows, heads * VDIM), bf16)),
        ("y", v((rows, model_width), f32)),
        ("give", v((others, halves, part, model_width // halves), bf16)),
        ("take", v((others, halves, part, model_width // halves), bf16)),
        ("load_sem", dma((10,))),
        ("kv_sem", dma((heads, 2))),
        ("tok_sem", dma((2, others))),
        ("klat_sem", dma((2, others))),
        ("qlat_sem", dma((2, others))),
        ("rim_sem", dma((2,))),
        ("ici_recv", dma((SPAN,))),
        ("core_send", dma((SPAN, others))),
        ("core_recv", dma((SPAN, others))),
        ("z_send", dma((layers,))),
        ("near_send", dma((layers,))),
        ("far_send", dma((2 * layers,))),
        ("y_sem", dma((2, others, halves))),
    ]
    if w_kvlat.shape[1] % LANES == 0 and w_qlat.shape[1] % LANES == 0:
        both_cols = w_kvlat.shape[1] + w_qlat.shape[1]
        scratch.append(("w_lat_v", v((model_width, both_cols), bf16)))
    else:
        scratch.append(("w_kvlat_v", v(w_kvlat.shape, bf16)))
        scratch.append(("w_qlat_v", v(w_qlat.shape, bf16)))
    names = [entry[0] for entry in inputs + outputs + scratch]
    layer_out, log_rows = pl.pallas_call(
        functools.partial(fused_kernel, names, seq_count),
        out_shape=tuple(entry[1] for entry in outputs),
        in_specs=[entry[2] for entry in inputs],
        out_specs=(vmem, vmem),
        scratch_shapes=[entry[1] for entry in scratch],
        compiler_params=pltpu.CompilerParams(
            vmem_limit_bytes=62 * 1024 * 1024, collective_id=0, has_side_effects=True
        ),
        cost_estimate=pl.CostEstimate(
            flops=30 * 10**9, bytes_accessed=2 * 10**7, transcendentals=10**7
        ),
    )(*[entry[1] for entry in inputs])
    return layer_out.astype(bf16), log_rows.T


def solution(mesh):
    in_specs = (
        P("sp", "tp"),
        P(),
        P(None, "tp"),
        P(None, "tp"),
        P(None, "tp"),
        P(),
        P(),
        P(),
        P(None, "tp"),
        P(None, "tp"),
        P(None, "tp"),
        P(None, "tp"),
        P(),
        P(),
        P("tp", None),
        P("tp", None),
    )
    out_specs = (P(("sp", "tp"), None), P("sp", "tp"))
    return jax.shard_map(
        per_device, mesh=mesh, in_specs=in_specs, out_specs=out_specs, check_vma=False
    )
```
